256 devices in a mesh: sp: 64 (over z, y, core), tp: 4 (over x).
Axes of the slice: x: 4, y: 4, z: 8, core: 2. Of those that a mesh axis runs over, the one named last changes fastest.
Arguments:
- queries: bfloat16 [32768, 1024], P('sp', 'tp'), may hold values from -6 to 6
- keys: bfloat16 [32768, 1024], P('sp', 'tp'), may hold values from -6 to 6
- values: bfloat16 [32768, 1024], P('sp', 'tp'), may hold values from -6 to 6
- output_gate_logits: bfloat16 [32768, 1024], P('sp', 'tp'), may hold values from -6 to 6
- input_gate_log: float32 [32768, 8], P('sp', 'tp'), may hold values from -5 to 125
- forget_gate_logits: float32 [32768, 8], P('sp', 'tp')
- extra_decay_log: float32 [32768, 8], P('sp', 'tp'), may hold values from -1 to 0
- document: int32 [32768], P('sp'), may hold values from 0 to 31, never falling along the last dimension, each value on 1 to 2048 neighbouring positions
- residual: bfloat16 [32768, 2048], P('sp', 'tp'), may hold values from -16 to 16
- cell_norm_gain: bfloat16 [1024], P('tp'), may hold values from 0.099609375 to 1.8984375
- output_weight: bfloat16 [1024, 2048], P('tp'), may hold values from -0.1875 to 0.1875
- mixer_norm_gain: bfloat16 [2048], P('tp'), may hold values from 0.099609375 to 1.8984375
- up_weight: bfloat16 [2048, 8192], P('sp', 'tp'), may hold values from -0.125 to 0.125
- down_weight: bfloat16 [8192, 2048], P('tp', 'sp'), may hold values from -0.0625 to 0.0625
Outputs:
- layer_out: bfloat16 [32768, 2048], P('sp', 'tp')
The draws below stay inside these ranges and needn't reach their ends.
All inputs are finite; a program needn't handle non-finite values.
Results may differ from the reference program's by a relative error of at most 0.015.
Values may be sent and summed in bfloat16 or wider, within the bound.
No kernel may reach another device: no remote copies, remote signals or barrier semaphores. Data moves between devices by JAX's collectives and lax.ppermute only.
A program may use at most 128 MiB of HBM per device.

```python
import math
import jax
import jax.numpy as jnp
import numpy as np
from jax import lax

D = 2048
FF = 8192
HM = 8
DH = 128
BLOCK = 128
TOK_DEV = 512
TOKENS = 32768
DOCS = 32
MOST = 2048
N_SP = 64
N_TP = 4


def draw_input_gate_log(key, part):
    key_base = jax.random.fold_in(key, 0)
    return jnp.clip(jax.random.normal(key_base, (TOKENS, HM), jnp.float32), -4.0, 4.0)


def draw_forget_gate_logits(key, part):
    key_kind, key_device, key_noise = jax.random.split(key, 3)
    fast_heads = jax.random.randint(key_kind, (HM,), 0, 2) == 1
    device_rate = jax.random.uniform(key_device, (TOKENS // TOK_DEV, 1, 1), jnp.float32, 0.0, math.log(4.0))
    jitter = jax.random.uniform(key_noise, (TOKENS // TOK_DEV, TOK_DEV, HM), jnp.float32, -0.7, 0.7)
    slow_pre = math.log(8.0 * MOST) - device_rate + jitter
    fast_pre = math.log(40.0) + jitter
    result = jnp.where(fast_heads[None, None, :], fast_pre, slow_pre)
    return result.reshape(TOKENS, HM)


def draw_extra_decay_log(key, part):
    key_spot, key_head, key_depth = jax.random.split(key, 3)
    places = max(TOKENS // TOK_DEV * 2, 4)
    spots = jax.random.randint(key_spot, (places,), 0, TOKENS)
    heads_hit = jax.random.randint(key_head, (places,), 0, HM)
    depths = jax.random.uniform(key_depth, (places,), jnp.float32, math.log(0.5), math.log(0.8))
    return jnp.zeros((TOKENS, HM), jnp.float32).at[spots, heads_hit].min(depths)


def draw_residual(key, part):
    key_values = jax.random.fold_in(key, 0)
    ramp = jnp.exp(jnp.linspace(0.0, math.log(3.0), D)).astype(jnp.float32)
    entries = jnp.clip(jax.random.normal(key_values, (TOKENS, D), jnp.float32), -4.0, 4.0)
    return (entries * ramp[None, :] / 1.7).astype(jnp.bfloat16)


def shard_levels(rng, dims, cuts, smallest, high):
    loudness = 1.0
    for axis_at, parts in cuts:
        draws = jax.random.uniform(jax.random.fold_in(jax.random.fold_in(rng, 6), axis_at), (parts,), jnp.float32, smallest / len(cuts), high / len(cuts))
        loudness = loudness * jnp.repeat(jnp.exp(draws), dims[axis_at] // parts).reshape((-1,) + (1,) * (len(dims) - 1 - axis_at))
    return loudness


def split_up(amount, total, most, slope):
    portions = [(1 << 20) // math.isqrt(grade ** slope) + 1 for grade in range(2, amount + 1)]
    surplus, counts = total - most - (amount - 1), [1] * (amount - 1)
    while surplus > 0:
        free = [i for i in range(amount - 1) if counts[i] < most]
        mass, budget = sum([portions[i] for i in free]), surplus
        for i in free:
            more = min(most - counts[i], max(1, budget * portions[i] // mass), surplus)
            counts[i] = counts[i] + more
            surplus = surplus - more
    return np.array([most] + counts)


def ragged_sizes(stream_key, count, total, limit, lean):
    if count == 2:
        one = jax.random.randint(stream_key, (), max(1, total - limit), min(limit, total - 1) + 1)
        return jnp.stack([one, total - one])
    lengths = jnp.asarray(split_up(count, total, limit, lean), jnp.int32)
    couples = (count - 1) // 2
    source_of, receiver = lengths[1:1 + 2 * couples:2], lengths[2:2 + 2 * couples:2]
    slack = jnp.minimum(source_of - 1, limit - receiver)
    passed = jax.random.randint(jax.random.fold_in(stream_key, 1), (couples,), 0, 1 << 20) % (slack + 1)
    lengths = lengths.at[1:1 + 2 * couples:2].set(source_of - passed).at[2:2 + 2 * couples:2].set(receiver + passed)
    return lengths[jax.random.permutation(jax.random.fold_in(stream_key, 2), count)]


def gaussian(key, extent, scale, bound, cuts=(), dtype=jnp.bfloat16):
    values = jax.random.normal(key, extent, jnp.float32) * scale
    if len(cuts) > 0:
        values = shard_levels(key, extent, cuts, -0.22, 0.18) * values
    return jnp.clip(values, min=-bound, max=bound).astype(dtype)


def setup_inputs(seed: int = 0) -> dict:
    streams_of = jax.random.split(jax.random.key(seed), 15)
    queries = gaussian(streams_of[0], (TOKENS, HM * DH), 1.0, 6.0, ((0, 64), (1, 4)))
    keys = gaussian(streams_of[1], (TOKENS, HM * DH), 1.0, 6.0, ((0, 64), (1, 4)))
    values = gaussian(streams_of[2], (TOKENS, HM * DH), 1.0, 6.0, ((0, 64), (1, 4)))
    output_gate_logits = gaussian(streams_of[3], (TOKENS, HM * DH), 1.0, 6.0, ((0, 64), (1, 4)))
    input_gate_log = draw_input_gate_log(jax.random.fold_in(streams_of[14], 71), 0)
    forget_gate_logits = draw_forget_gate_logits(jax.random.fold_in(streams_of[14], 71), 0)
    extra_decay_log = draw_extra_decay_log(jax.random.fold_in(streams_of[14], 71), 0)
    document = jnp.searchsorted(jnp.cumsum(ragged_sizes(streams_of[7], DOCS, TOKENS, MOST, 0)), jnp.arange(TOKENS), side="right").astype(jnp.int32)
    residual = draw_residual(jax.random.fold_in(streams_of[14], 71), 0)
    cell_norm_gain = jnp.clip(1.0 + 0.18 * jax.random.normal(streams_of[9], (HM * DH,), jnp.float32), 0.099609375, 1.8984375).astype(jnp.bfloat16)
    output_weight = gaussian(streams_of[10], (HM * DH, D), (HM * DH) ** -0.5, 0.1875, ((0, 4),))
    mixer_norm_gain = jnp.clip(1.0 + 0.18 * jax.random.normal(streams_of[11], (D,), jnp.float32), 0.099609375, 1.8984375).astype(jnp.bfloat16)
    up_weight = gaussian(streams_of[12], (D, FF), D ** -0.5, 0.125, ((0, 64), (1, 4)))
    down_weight = gaussian(streams_of[13], (FF, D), FF ** -0.5, 0.0625, ((0, 4), (1, 64)))
    return dict(queries=queries, keys=keys, values=values, output_gate_logits=output_gate_logits, input_gate_log=input_gate_log, forget_gate_logits=forget_gate_logits, extra_decay_log=extra_decay_log, document=document, residual=residual, cell_norm_gain=cell_norm_gain, output_weight=output_weight, mixer_norm_gain=mixer_norm_gain, up_weight=up_weight, down_weight=down_weight)


NEG = -1e+30
EPS = 1e-06
HIGH = lax.Precision.HIGHEST

def block_terms(carry, inputs):
    memory, normer, stabil, last_doc = carry
    q_blk, k_blk, v_blk, gate_in, gate_log, doc_blk = inputs
    length = doc_blk.shape[0]
    causal = jnp.arange(length)[:, None] >= jnp.arange(length)[None, :]
    cumulative = jnp.cumsum(gate_log, axis=-1)
    same_doc = (doc_blk[:, None] == doc_blk[None, :]) & causal
    pair_log = cumulative[:, :, None] - cumulative[:, None, :] + gate_in[:, None, :]
    pair_log = jnp.where(same_doc[None], pair_log, NEG)
    live_rows = doc_blk == last_doc
    carried_log = jnp.where(live_rows[None, :], cumulative + stabil[:, None], NEG)
    peak_log = jnp.maximum(carried_log, lax.optimization_barrier(jnp.max(pair_log, axis=-1)))
    weights = jnp.exp(pair_log - peak_log[:, :, None])
    carried = jnp.exp(carried_log - peak_log)
    scores = jnp.einsum('htd,hsd->hts', q_blk, k_blk, precision=HIGH) * weights
    numerator = carried[:, :, None] * jnp.einsum('htd,hde->hte', q_blk, memory, precision=HIGH)
    numerator = numerator + jnp.einsum('hts,hse->hte', scores, v_blk, precision=HIGH)
    denominator = carried * jnp.einsum('htd,hd->ht', q_blk, normer, precision=HIGH) + lax.optimization_barrier(jnp.sum(scores, axis=-1))
    end_doc = doc_blk[-1]
    end_cum = cumulative[:, -1]
    keep_log = jnp.where((doc_blk == end_doc)[None, :], end_cum[:, None] - cumulative + gate_in, NEG)
    old_log = jnp.where(last_doc == end_doc, end_cum + stabil, NEG)
    new_stab = jnp.maximum(old_log, lax.optimization_barrier(jnp.max(keep_log, axis=-1)))
    scaled = jnp.exp(keep_log - new_stab[:, None])
    decayed = jnp.exp(old_log - new_stab)
    memory = decayed[:, None, None] * memory + jnp.einsum('hs,hsd,hse->hde', scaled, k_blk, v_blk, precision=HIGH)
    normer = decayed[:, None] * normer + jnp.einsum('hs,hsd->hd', scaled, k_blk, precision=HIGH)
    return ((memory, normer, new_stab, end_doc), (numerator, denominator, peak_log, cumulative))

def split_heads(source, blocks):
    return source.astype(jnp.float32).reshape(blocks, BLOCK, -1, DH).transpose(0, 2, 1, 3)

def split_gates(source, blocks):
    return source.reshape(blocks, BLOCK, -1).transpose(0, 2, 1)

def within_block_pass(queries, keys, values, input_gate_log, forget_gate_logits, extra_decay_log, document):
    blocks = queries.shape[0] // BLOCK
    head_count = queries.shape[1] // DH
    query_heads = split_heads(queries, blocks) * DH ** (-0.5)
    forget_log_values = jax.nn.log_sigmoid(forget_gate_logits) + extra_decay_log
    inputs = (query_heads, split_heads(keys, blocks), split_heads(values, blocks), split_gates(input_gate_log, blocks), split_gates(forget_log_values, blocks), document.reshape(blocks, BLOCK))
    initial = (jnp.zeros((head_count, DH, DH), jnp.float32), jnp.zeros((head_count, DH), jnp.float32), jnp.full((head_count,), NEG, jnp.float32), jnp.array(-1, jnp.int32))
    final_state, output_rows = lax.scan(block_terms, initial, inputs)
    return (query_heads, final_state, output_rows)

def head_mix(cell_out, output_gate_logits, cell_norm_gain):
    row_count = output_gate_logits.shape[0]
    head_count = cell_out.shape[1]
    hidden = cell_out.transpose(0, 2, 1, 3).reshape(row_count, head_count * DH)
    inverse = lax.rsqrt(lax.optimization_barrier(jnp.mean(hidden * hidden, axis=1, keepdims=True)) + EPS)
    gated = jax.nn.sigmoid(output_gate_logits.astype(jnp.float32))
    gains = cell_norm_gain.astype(jnp.float32)
    return (gated * hidden * inverse * gains[None, :]).astype(jnp.bfloat16)

def reference(queries, keys, values, output_gate_logits, input_gate_log, forget_gate_logits, extra_decay_log, document, residual, cell_norm_gain, output_weight, mixer_norm_gain, up_weight, down_weight):
    query_heads, final_state, output_rows = within_block_pass(queries, keys, values, input_gate_log, forget_gate_logits, extra_decay_log, document)
    numerator, denominator, peak_log, cumulative = output_rows
    cell_out = numerator / jnp.maximum(jnp.abs(denominator), 1.0)[..., None]
    mixed = head_mix(cell_out, output_gate_logits, cell_norm_gain)
    out_groups = output_weight.reshape(N_TP, -1, D).astype(jnp.float32)
    down_groups = down_weight.reshape(N_TP, -1, D).astype(jnp.float32)
    gain_wide = mixer_norm_gain.astype(jnp.float32)

    def rows_step(row_args):
        mixed_rows, resid_rows = row_args
        row_count = mixed_rows.shape[0]
        group_parts = jnp.einsum('rgk,gkd->grd', mixed_rows.reshape(row_count, N_TP, -1).astype(jnp.float32), out_groups)
        group_parts = lax.optimization_barrier(group_parts.astype(jnp.bfloat16)).astype(jnp.float32)
        first_sum = (resid_rows.astype(jnp.float32) + lax.optimization_barrier(jnp.sum(group_parts, axis=0))).astype(jnp.bfloat16)
        first_wide = lax.optimization_barrier(first_sum).astype(jnp.float32)
        inverse = lax.rsqrt(lax.optimization_barrier(jnp.mean(first_wide * first_wide, axis=1, keepdims=True)) + EPS)
        normed = (first_wide * inverse * gain_wide).astype(jnp.bfloat16)
        hidden = jnp.dot(normed, up_weight, preferred_element_type=jnp.float32)
        squared = jnp.square(jax.nn.relu(hidden)).astype(jnp.bfloat16)
        channel_parts = jnp.einsum('rgf,gfd->grd', squared.reshape(row_count, N_TP, -1).astype(jnp.float32), down_groups)
        channel_parts = lax.optimization_barrier(channel_parts.astype(jnp.bfloat16)).astype(jnp.float32)
        return (first_wide + lax.optimization_barrier(jnp.sum(channel_parts, axis=0))).astype(jnp.bfloat16)
    layer = lax.map(rows_step, (mixed.reshape(N_SP, -1, mixed.shape[1]), residual.reshape(N_SP, -1, D)))
    return layer.reshape(-1, D)
```

```python
import jax
import jax.numpy as jnp
from jax import lax
from jax.experimental import pallas as pl
from jax.experimental.pallas import tpu as pltpu
from jax.sharding import Mesh
from jax.sharding import PartitionSpec as P

NEG = -1e30
EPS = 1e-06
DH = 128
BLK = 128
NB = 4
HD = 2
TOK = 512
OWN = 128
D = 2048
FF = 2048
SCALE = DH ** (-0.5)
BF = jnp.bfloat16
F32 = jnp.float32
HIGH = lax.Precision.HIGHEST
SP = ("z", "y", "c")
REL = (0, -1, 1, 2)


def shift(value, axis, by):
    count = lax.axis_size(axis)
    return lax.ppermute(value, axis, [(i, (i + by) % count) for i in range(count)])


def shift_sp(value, by):
    return lax.ppermute(value, SP, [(i, i + by) for i in range(64 - by)])


def split3(value):
    hi = value.astype(BF)
    rest = value - hi.astype(F32)
    mid = rest.astype(BF)
    low = (rest - mid.astype(F32)).astype(BF)
    return hi, mid, low


def block_sums(gates):
    tri = (
        lax.broadcasted_iota(jnp.int32, (BLK, BLK), 0)
        <= lax.broadcasted_iota(jnp.int32, (BLK, BLK), 1)
    ).astype(F32)
    cum = jnp.dot(gates[8:16, :], tri, precision=HIGH, preferred_element_type=F32)
    totals = [cum[r : r + 1, BLK - 1 : BLK] for r in range(8)]
    return cum, totals


def summary_kernel(gates_ref, k_ref, v_ref, out_ref):
    gates = gates_ref[...]
    cum, totals = block_sums(gates)
    docs = gates[16:24, :]
    last_doc = docs[3:4, BLK - 1 : BLK]
    rows, stabs, sums = [], [], []
    for h in range(HD):
        keeps = []
        after = jnp.zeros((1, 1), F32)
        for b in reversed(range(NB)):
            r = h * NB + b
            keep = (totals[r] - cum[r : r + 1, :]) + after + gates[r : r + 1, :]
            keeps.append(jnp.where(docs[b : b + 1, :] == last_doc, keep, NEG))
            after = after + totals[r]
        keeps = keeps[::-1]
        stab = jnp.max(keeps[0], axis=1, keepdims=True)
        for keep in keeps[1:]:
            stab = jnp.maximum(stab, jnp.max(keep, axis=1, keepdims=True))
        rows += [jnp.exp(keep - stab) for keep in keeps]
        stabs.append(stab)
        sums.append(after)
    columns = jnp.transpose(jnp.concatenate(rows, axis=0))
    norms = []
    for h in range(HD):
        scaled = jnp.concatenate(
            [
                k_ref[b * BLK : (b + 1) * BLK, h * DH : (h + 1) * DH].astype(F32)
                * columns[:, h * NB + b : h * NB + b + 1]
                for b in range(NB)
            ],
            axis=0,
        )
        norms.append(jnp.sum(scaled, axis=0, keepdims=True))
        memory = lax.dot_general(
            scaled.astype(BF),
            v_ref[:, h * DH : (h + 1) * DH],
            (((0,), (0,)), ((), ())),
            preferred_element_type=F32,
        )
        out_ref[h * DH : (h + 1) * DH, :] = memory.astype(BF)
    wide = lambda a: jnp.broadcast_to(a, (1, BLK))
    small = jnp.concatenate(
        norms
        + [wide(a) for a in stabs]
        + [wide(a) for a in sums]
        + [wide(last_doc + 1.0), jnp.zeros((1, BLK), F32)],
        axis=0,
    )
    hi, mid, low = split3(small)
    pad = jnp.zeros((8, BLK), F32)
    out_ref[256:272, :] = jnp.concatenate([hi.astype(F32), mid.astype(F32)], axis=0).astype(BF)
    out_ref[272:288, :] = jnp.concatenate([low.astype(F32), pad], axis=0).astype(BF)


def local_kernel(gates_ref, q_ref, k_ref, v_ref, numer_ref, aux_ref):
    gates = gates_ref[...]
    cum, totals = block_sums(gates)
    docs = gates[16:24, :]
    cum_cols = jnp.transpose(cum)
    doc_cols = jnp.transpose(docs)
    for b in range(NB):
        width = (b + 1) * BLK
        row_at = lax.broadcasted_iota(jnp.int32, (BLK, width), 0) + b * BLK
        col_at = lax.broadcasted_iota(jnp.int32, (BLK, width), 1)
        doc_row = jnp.concatenate([docs[a : a + 1, :] for a in range(b + 1)], axis=1)
        mask = (doc_cols[:, b : b + 1] == doc_row) & (col_at <= row_at)
        peaks, denoms = [], []
        for h in range(HD):
            r = h * NB + b
            parts = [gates[r : r + 1, :] - cum[r : r + 1, :]]
            between = jnp.zeros((1, 1), F32)
            for a in reversed(range(b)):
                ra = h * NB + a
                parts.append((totals[ra] - cum[ra : ra + 1, :]) + between + gates[ra : ra + 1, :])
                between = between + totals[ra]
            source = jnp.concatenate(parts[::-1], axis=1)
            pair = jnp.where(mask, cum_cols[:, r : r + 1] + source, NEG)
            peak = jnp.max(pair, axis=1, keepdims=True)
            lanes = slice(h * DH, (h + 1) * DH)
            scores = lax.dot_general(
                q_ref[b * BLK : (b + 1) * BLK, lanes],
                k_ref[0:width, lanes],
                (((1,), (1,)), ((), ())),
                preferred_element_type=F32,
            )
            scores = scores * SCALE * jnp.exp(pair - peak)
            denoms.append(jnp.sum(scores, axis=1, keepdims=True))
            peaks.append(peak)
            numer_ref[b * BLK : (b + 1) * BLK, lanes] = jnp.dot(
                scores.astype(BF), v_ref[0:width, lanes], preferred_element_type=F32
            )
        lane = lax.broadcasted_iota(jnp.int32, (BLK, BLK), 1)
        aux = jnp.where(
            lane == 0,
            peaks[0],
            jnp.where(lane == 1, peaks[1], jnp.where(lane == 2, denoms[0], denoms[1])),
        )
        aux_ref[b * BLK : (b + 1) * BLK, :] = aux


def combine_kernel(
    at_ref, gates_ref, q_ref, og_ref, gain_ref, numer_ref, aux_ref, s1, s2, s3, s4, *rest
):
    outs, full_ref = rest[:4], rest[4]
    gates = gates_ref[...]
    cum, totals = block_sums(gates)
    docs = gates[16:24, :]
    cum_cols = jnp.transpose(cum)
    doc_cols = jnp.transpose(docs)
    doc0 = docs[0:1, 0:1]
    smalls = []
    for s in (s1, s2, s3, s4):
        upper = s[256:272, :].astype(F32)
        lower = s[272:288, :].astype(F32)
        smalls.append(upper[0:8, :] + upper[8:16, :] + lower[0:8, :])
    states = []
    for h in range(HD):
        far = jnp.zeros((1, 1), F32)
        logs, valids = [], []
        for small in smalls:
            valid = small[6:7, 0:1] == doc0 + 1.0
            logs.append(jnp.where(valid, small[2 + h : 3 + h, 0:1] + far, NEG))
            valids.append(valid)
            far = far + small[4 + h : 5 + h, 0:1]
        stab = jnp.maximum(jnp.maximum(logs[0], logs[1]), jnp.maximum(logs[2], logs[3]))
        memory = jnp.zeros((DH, DH), F32)
        normer = jnp.zeros((1, DH), F32)
        for s, small, log, valid in zip((s1, s2, s3, s4), smalls, logs, valids):
            weight = jnp.where(valid, jnp.exp(log - stab), 0.0)
            memory = memory + weight * s[h * DH : (h + 1) * DH, :].astype(F32)
            normer = normer + weight * small[h : h + 1, :]
        states.append((memory.astype(BF), normer, stab))
    before = [jnp.zeros((1, 1), F32) for _ in range(HD)]
    for b in range(NB):
        rows = slice(b * BLK, (b + 1) * BLK)
        live = doc_cols[:, b : b + 1] == doc0
        aux = aux_ref[rows, :]
        squares = jnp.zeros((BLK, 1), F32)
        for h in range(HD):
            lanes = slice(h * DH, (h + 1) * DH)
            memory, normer, stab = states[h]
            r = h * NB + b
            carried = jnp.where(
                live & (stab > 0.5 * NEG), cum_cols[:, r : r + 1] + (before[h] + stab), NEG
            )
            peak = aux[:, h : h + 1]
            merged = jnp.maximum(peak, carried)
            own_w = jnp.exp(peak - merged)
            far_w = jnp.exp(carried - merged) * SCALE
            q_blk = q_ref[rows, lanes]
            numer = own_w * numer_ref[rows, lanes] + far_w * jnp.dot(
                q_blk, memory, preferred_element_type=F32
            )
            denom = own_w * aux[:, 2 + h : 3 + h] + far_w * jnp.sum(
                q_blk.astype(F32) * normer, axis=1, keepdims=True
            )
            cell = numer / jnp.maximum(jnp.abs(denom), 1.0)
            squares = squares + jnp.sum(cell * cell, axis=1, keepdims=True)
            gate = jax.nn.sigmoid(og_ref[rows, lanes].astype(F32))
            full_ref[rows, lanes] = (gate * cell * gain_ref[0:1, lanes].astype(F32)).astype(BF)
            before[h] = before[h] + totals[r]
        hi, mid, low = split3(squares)
        lane = lax.broadcasted_iota(jnp.int32, (BLK, BLK), 1)
        pieces = jnp.where(
            lane == 0,
            hi.astype(F32),
            jnp.where(lane == 1, mid.astype(F32), jnp.where(lane == 2, low.astype(F32), 0.0)),
        )
        full_ref[rows, 256:384] = pieces.astype(BF)
    x = at_ref[3]
    for out, rel in zip(outs, REL):
        start = pl.multiple_of(lax.rem(x + rel + 4, 4) * OWN, OWN)
        out[...] = full_ref[pl.ds(start, OWN), :]


def project_kernel(at_ref, *refs):
    cells = refs[0:4]
    resids = refs[4:8]
    own_w = refs[8]
    mine = refs[9:12]
    other = refs[12:15]
    first_ref, normed_ref, w_ref, g_ref, r_ref, sem = refs[15:]
    core = at_ref[2]
    x = at_ref[3]
    copies = [pltpu.make_async_copy(own_w, w_ref.at[pl.ds(0, 256)], sem)]
    for k in range(3):
        for part, half in ((mine[k], core), (other[k], 1 - core)):
            start = pl.multiple_of((k + 1) * 256 + half * 128, 128)
            copies.append(pltpu.make_async_copy(part, w_ref.at[pl.ds(start, 128)], sem))
    for copy in copies:
        copy.start()
    squares = jnp.zeros((OWN, 1), F32)
    for k, rel in enumerate(REL):
        g_ref[:, k * 256 : (k + 1) * 256] = cells[k][:, 0:256]
        sent = cells[k][:, 256:384].astype(F32)
        squares = squares + (sent[:, 0:1] + sent[:, 1:2] + sent[:, 2:3])
        r_ref[lax.rem(x + rel + 4, 4)] = resids[k][...]
    inverse = lax.rsqrt(squares / 1024.0 + EPS)
    for copy in copies:
        copy.wait()
    total = jnp.zeros((OWN, 1), F32)
    for a in range(4):
        cols = slice(a * 512, (a + 1) * 512)
        head = jnp.dot(g_ref[...], w_ref[:, cols], preferred_element_type=F32) * inverse
        first = (r_ref[a, 0:OWN, :].astype(F32) + head).astype(BF)
        first_ref[:, cols] = first
        wide = first.astype(F32)
        total = total + jnp.sum(wide * wide, axis=1, keepdims=True)
    inverse = lax.rsqrt(total / float(D) + EPS)
    for a in range(4):
        cols = slice(a * 512, (a + 1) * 512)
        gain = r_ref[a, OWN : OWN + 16, :].astype(F32)[0:1, :]
        normed_ref[:, cols] = (first_ref[:, cols].astype(F32) * inverse * gain).astype(BF)


def place(z, y, c):
    return pl.multiple_of((lax.rem(z + 16, 8) * 8 + lax.rem(y + 8, 4) * 2 + c) * 32, 32)


def up_copies(at_ref, pieces, w_ref, sem):
    z, y, c = at_ref[0], at_ref[1], at_ref[2]
    copies = []
    for part, core in ((pieces[:9], c), (pieces[9:], 1 - c)):
        for piece, dz in zip(part[:7], (0, -1, 1, -2, 2, -3, 3)):
            for k, dy in enumerate(REL):
                dst = place(z + dz, y + dy, core)
                copies.append((piece.at[pl.ds(k * 32, 32)], dst))
        for k, dy in enumerate(REL):
            dst = place(z + 4, y + dy, core)
            copies.append((part[7 + k // 2].at[pl.ds((k % 2) * 32, 32)], dst))
    return [pltpu.make_async_copy(src, w_ref.at[pl.ds(dst, 32)], sem) for src, dst in copies]


def down_copies(at_ref, pieces, w_ref, sem):
    z, y, c = at_ref[0], at_ref[1], at_ref[2]
    copies = []

    def spread(src, start, dy, core, subs):
        at = start
        for dz, extra, rows in subs:
            dst = place(z + dz, y + dy, core) + extra
            copies.append((src.at[pl.ds(at, rows)], pl.multiple_of(dst, 16), rows))
            at += rows

    first = [(0, 0, 32), (-1, 0, 32), (1, 0, 32), (-2, 0, 32)]
    second = [(2, 0, 32), (-3, 0, 32), (3, 0, 32), (4, 0, 16), (4, 16, 16)]
    for part, core in ((pieces[:5], c), (pieces[5:], 1 - c)):
        for piece, dy in zip(part[:3], (0, -1, 1)):
            spread(piece, 0, dy, core, first + second)
        spread(part[3], 0, 2, core, first)
        spread(part[4], 0, 2, core, second)
    return [
        pltpu.make_async_copy(src, w_ref.at[pl.ds(dst, rows)], sem) for src, dst, rows in copies
    ]


def up_kernel(at_ref, n0, n1, n2, n3, *refs):
    pieces = refs[:18]
    out_ref, w_ref, x_ref, sem = refs[18:]
    copies = up_copies(at_ref, pieces, w_ref, sem)
    for copy in copies:
        copy.start()
    for k, n in enumerate((n0, n1, n2, n3)):
        x_ref[k * OWN : (k + 1) * OWN, :] = n[...]
    for copy in copies:
        copy.wait()
    for a in range(4):
        cols = slice(a * 512, (a + 1) * 512)
        hidden = jnp.dot(x_ref[...], w_ref[:, cols], preferred_element_type=F32)
        out_ref[:, cols] = jnp.square(jnp.maximum(hidden, 0.0)).astype(BF)


def down_kernel(at_ref, sq_ref, first_ref, *refs):
    pieces = refs[:10]
    outs, w_ref, sem = refs[10:14], refs[14], refs[15]
    x = at_ref[3]
    copies = down_copies(at_ref, pieces, w_ref, sem)
    for copy in copies:
        copy.start()
    for copy in copies:
        copy.wait()
    for out, rel in zip(outs, REL):
        block = lax.rem(x + rel + 4, 4)
        start = pl.multiple_of(block * 512, 512)
        part = lax.dot_general(
            sq_ref[...],
            w_ref[pl.ds(start, 512), :],
            (((1,), (1,)), ((), ())),
            preferred_element_type=F32,
        )
        out[0:OWN, :] = (part[0:OWN, :] + first_ref[block].astype(F32)).astype(BF)
        out[OWN:TOK, :] = part[OWN:TOK, :].astype(BF)


def sum_kernel(at_ref, p0, p1, p2, p3, out_ref):
    x = at_ref[3]
    for a in range(4):
        total = jnp.zeros((OWN, 512), F32)
        for piece, rel in zip((p0, p1, p2, p3), REL):
            offset = lax.rem(a - (x + rel) + 8, 4)
            slot = jnp.where(offset == 0, 0, jnp.where(offset == 3, 1, jnp.where(offset == 1, 2, 3)))
            total = total + piece[pl.ds(pl.multiple_of(slot * OWN, OWN), OWN), :].astype(F32)
        out_ref[a * OWN : (a + 1) * OWN, :] = total.astype(BF)


def smem():
    return pl.BlockSpec(memory_space=pltpu.SMEM)


def vmem():
    return pl.BlockSpec(memory_space=pltpu.VMEM)


def hbm():
    return pl.BlockSpec(memory_space=pl.ANY)


def shape(*dims, dtype=BF):
    return jax.ShapeDtypeStruct(dims, dtype)


def call(body, name, specs, outs, scratch=(), flops=0):
    many = isinstance(outs, (list, tuple))
    return pl.pallas_call(
        body,
        name=name,
        in_specs=specs,
        out_specs=[vmem() for _ in outs] if many else vmem(),
        out_shape=outs,
        scratch_shapes=list(scratch),
        compiler_params=pltpu.CompilerParams(vmem_limit_bytes=56 * 1024 * 1024),
        cost_estimate=pl.CostEstimate(flops=flops, bytes_accessed=0, transcendentals=0),
    )


def gather_up(own):
    blk = jnp.concatenate(
        [own, shift(own, "y", 1), shift(own, "y", -1), shift(own, "y", 2)], axis=0
    )
    p1, m1 = shift(blk, "z", 1), shift(blk, "z", -1)
    p2, m2 = shift(p1, "z", 1), shift(m1, "z", -1)
    p3, m3 = shift(p2, "z", 1), shift(m2, "z", -1)
    p4, m4 = shift(p3[:64], "z", 1), shift(m3[64:], "z", -1)
    mine = [blk, p1, m1, p2, m2, p3, m3, p4, m4]
    return mine + [shift(a, "c", 1) for a in mine]


def gather_down(own):
    p1, m1 = shift(own, "z", 1), shift(own, "z", -1)
    p2, m2 = shift(p1, "z", 1), shift(m1, "z", -1)
    p3, m3 = shift(p2, "z", 1), shift(m2, "z", -1)
    p4, m4 = shift(p3[:16], "z", 1), shift(m3[16:], "z", -1)
    blk = jnp.concatenate([own, p1, m1, p2, m2, p3, m3, p4, m4], axis=0)
    q1, q2 = shift(blk, "y", 1), shift(blk, "y", -1)
    q3, q4 = shift(q1[:128], "y", 1), shift(q2[128:], "y", -1)
    mine = [blk, q1, q2, q3, q4]
    return mine + [shift(a, "c", 1) for a in mine]


def local(
    queries,
    keys,
    values,
    output_gate_logits,
    input_gate_log,
    forget_gate_logits,
    extra_decay_log,
    document,
    residual,
    cell_norm_gain,
    output_weight,
    mixer_norm_gain,
    up_weight,
    down_weight,
):
    z, y, c, x = (lax.axis_index(a) for a in ("z", "y", "c", "x"))
    at = jnp.stack([z, y, c, x]).astype(jnp.int32)

    forget_log = jax.nn.log_sigmoid(forget_gate_logits) + extra_decay_log
    docs = document.astype(F32).reshape(NB, BLK)
    gates = jnp.concatenate(
        [input_gate_log.T.reshape(8, BLK), forget_log.T.reshape(8, BLK), docs, docs], axis=0
    )

    state = call(
        summary_kernel, "summary", [vmem()] * 3, shape(288, DH), flops=2 * 2 * 512 * 128 * 128
    )(gates, keys, values)
    states = [shift_sp(state, by) for by in (1, 2, 3, 4)]

    gain_rows = jnp.broadcast_to(mixer_norm_gain[None, :], (16, 512))

    def own_rows(rel):
        rows = lax.dynamic_slice(residual, (lax.rem(x + rel + 4, 4) * OWN, 0), (OWN, 512))
        return jnp.concatenate([rows, gain_rows], axis=0)

    resids = [own_rows(0)]
    resids += [shift(own_rows(-by), "x", -by) for by in (-1, 1)]
    resids += [shift(own_rows(2), "x", 2)]

    half = lax.dynamic_slice(output_weight, (c * 128, 0), (128, D))
    mine_w = [shift(half, "x", 1), shift(half, "x", -1), shift(half, "x", 2)]
    other_w = [shift(w, "c", 1) for w in mine_w]

    ups = gather_up(up_weight)
    downs = gather_down(down_weight.T)

    numer, aux = call(
        local_kernel,
        "within",
        [vmem()] * 4,
        [shape(TOK, 256, dtype=F32), shape(TOK, BLK, dtype=F32)],
        flops=4 * 2 * 10 * 128**3,
    )(gates, queries, keys, values)
    cells = call(
        combine_kernel,
        "combine",
        [smem()] + [vmem()] * 10,
        [shape(OWN, 384)] * 4,
        [pltpu.VMEM((TOK, 384), BF)],
        flops=2 * 2 * 512 * 128 * 128,
    )(
        at,
        gates,
        queries,
        output_gate_logits,
        cell_norm_gain[None, :],
        numer,
        aux,
        *states,
    )
    got = [cells[0], shift(cells[2], "x", 1), shift(cells[1], "x", -1), shift(cells[3], "x", 2)]

    first, normed = call(
        project_kernel,
        "project",
        [smem()] + [vmem()] * 8 + [hbm()] * 7,
        [shape(OWN, D), shape(OWN, D)],
        [
            pltpu.VMEM((1024, D), BF),
            pltpu.VMEM((OWN, 1024), BF),
            pltpu.VMEM((4, OWN + 16, 512), BF),
            pltpu.SemaphoreType.DMA,
        ],
        flops=2 * 128 * 1024 * 2048,
    )(at, *got, *resids, output_weight, *mine_w, *other_w)

    wide = [normed, shift(normed, "x", 1), shift(normed, "x", -1), shift(normed, "x", 2)]
    squared = call(
        up_kernel,
        "up",
        [smem()] + [vmem()] * 4 + [hbm()] * 18,
        shape(TOK, FF),
        [pltpu.VMEM((D, FF), BF), pltpu.VMEM((TOK, D), BF), pltpu.SemaphoreType.DMA],
        flops=2 * 512 * 2048 * 2048,
    )(at, *wide, *ups)

    first_blocks = jnp.moveaxis(first.reshape(OWN, 4, 512), 1, 0)
    parts = call(
        down_kernel,
        "down",
        [smem()] + [vmem()] * 2 + [hbm()] * 10,
        [shape(TOK, 512)] * 4,
        [pltpu.VMEM((D, FF), BF), pltpu.SemaphoreType.DMA],
        flops=2 * 512 * 2048 * 2048,
    )(at, squared, first_blocks, *downs)
    got = [parts[0], shift(parts[2], "x", 1), shift(parts[1], "x", -1), shift(parts[3], "x", 2)]
    return call(sum_kernel, "total", [smem()] + [vmem()] * 4, shape(TOK, 512))(at, *got)


def solution(mesh):
    split = Mesh(mesh.devices.reshape(8, 4, 2, 4), ("z", "y", "c", "x"))
    return jax.shard_map(
        local,
        mesh=split,
        in_specs=(
            P(SP, "x"),
            P(SP, "x"),
            P(SP, "x"),
            P(SP, "x"),
            P(SP, "x"),
            P(SP, "x"),
            P(SP, "x"),
            P(SP),
            P(SP, "x"),
            P("x"),
            P("x", None),
            P("x"),
            P(SP, "x"),
            P("x", SP),
        ),
        out_specs=P(SP, "x"),
        check_vma=False,
    )
```

```python
import jax
import jax.numpy as jnp
from jax import lax
from jax.experimental import pallas as pl
from jax.experimental.pallas import tpu as pltpu
from jax.sharding import Mesh
from jax.sharding import PartitionSpec as P

NEG = -1e30
EPS = 1e-06
DH = 128
BLK = 128
NB = 4
HD = 2
TOK = 512
OWN = 128
D = 2048
FF = 2048
SCALE = DH ** (-0.5)
BF = jnp.bfloat16
F32 = jnp.float32
HIGH = lax.Precision.HIGHEST
SP = ("z", "y", "c")
REL = (0, -1, 1, 2)


def shift(value, axis, by):
    count = lax.axis_size(axis)
    return lax.ppermute(value, axis, [(i, (i + by) % count) for i in range(count)])


def shift_sp(value, by):
    return lax.ppermute(value, SP, [(i, i + by) for i in range(64 - by)])


def split3(value):
    hi = value.astype(BF)
    rest = value - hi.astype(F32)
    mid = rest.astype(BF)
    low = (rest - mid.astype(F32)).astype(BF)
    return hi, mid, low


def block_sums(gates):
    tri = (
        lax.broadcasted_iota(jnp.int32, (BLK, BLK), 0)
        <= lax.broadcasted_iota(jnp.int32, (BLK, BLK), 1)
    ).astype(F32)
    cum = jnp.dot(gates[8:16, :], tri, precision=HIGH, preferred_element_type=F32)
    totals = [cum[r : r + 1, BLK - 1 : BLK] for r in range(8)]
    return cum, totals


def summary_kernel(gates_ref, k_ref, v_ref, out_ref):
    gates = gates_ref[...]
    cum, totals = block_sums(gates)
    docs = gates[16:24, :]
    last_doc = docs[3:4, BLK - 1 : BLK]
    rows, stabs, sums = [], [], []
    for h in range(HD):
        keeps = []
        after = jnp.zeros((1, 1), F32)
        for b in reversed(range(NB)):
            r = h * NB + b
            keep = (totals[r] - cum[r : r + 1, :]) + after + gates[r : r + 1, :]
            keeps.append(jnp.where(docs[b : b + 1, :] == last_doc, keep, NEG))
            after = after + totals[r]
        keeps = keeps[::-1]
        stab = jnp.max(keeps[0], axis=1, keepdims=True)
        for keep in keeps[1:]:
            stab = jnp.maximum(stab, jnp.max(keep, axis=1, keepdims=True))
        rows += [jnp.exp(keep - stab) for keep in keeps]
        stabs.append(stab)
        sums.append(after)
    columns = jnp.transpose(jnp.concatenate(rows, axis=0))
    norms = []
    for h in range(HD):
        scaled = jnp.concatenate(
            [
                k_ref[b * BLK : (b + 1) * BLK, h * DH : (h + 1) * DH].astype(F32)
                * columns[:, h * NB + b : h * NB + b + 1]
                for b in range(NB)
            ],
            axis=0,
        )
        norms.append(jnp.sum(scaled, axis=0, keepdims=True))
        memory = lax.dot_general(
            scaled.astype(BF),
            v_ref[:, h * DH : (h + 1) * DH],
            (((0,), (0,)), ((), ())),
            preferred_element_type=F32,
        )
        out_ref[h * DH : (h + 1) * DH, :] = memory.astype(BF)
    wide = lambda a: jnp.broadcast_to(a, (1, BLK))
    small = jnp.concatenate(
        norms
        + [wide(a) for a in stabs]
        + [wide(a) for a in sums]
        + [wide(last_doc + 1.0), jnp.zeros((1, BLK), F32)],
        axis=0,
    )
    hi, mid, low = split3(small)
    pad = jnp.zeros((8, BLK), F32)
    out_ref[256:272, :] = jnp.concatenate([hi.astype(F32), mid.astype(F32)], axis=0).astype(BF)
    out_ref[272:288, :] = jnp.concatenate([low.astype(F32), pad], axis=0).astype(BF)


def local_kernel(gates_ref, q_ref, k_ref, v_ref, numer_ref, aux_ref):
    gates = gates_ref[...]
    cum, totals = block_sums(gates)
    docs = gates[16:24, :]
    cum_cols = jnp.transpose(cum)
    doc_cols = jnp.transpose(docs)
    for b in range(NB):
        width = (b + 1) * BLK
        row_at = lax.broadcasted_iota(jnp.int32, (BLK, width), 0) + b * BLK
        col_at = lax.broadcasted_iota(jnp.int32, (BLK, width), 1)
        doc_row = jnp.concatenate([docs[a : a + 1, :] for a in range(b + 1)], axis=1)
        mask = (doc_cols[:, b : b + 1] == doc_row) & (col_at <= row_at)
        peaks, denoms = [], []
        for h in range(HD):
            r = h * NB + b
            parts = [gates[r : r + 1, :] - cum[r : r + 1, :]]
            between = jnp.zeros((1, 1), F32)
            for a in reversed(range(b)):
                ra = h * NB + a
                parts.append((totals[ra] - cum[ra : ra + 1, :]) + between + gates[ra : ra + 1, :])
                between = between + totals[ra]
            source = jnp.concatenate(parts[::-1], axis=1)
            pair = jnp.where(mask, cum_cols[:, r : r + 1] + source, NEG)
            peak = jnp.max(pair, axis=1, keepdims=True)
            lanes = slice(h * DH, (h + 1) * DH)
            scores = lax.dot_general(
                q_ref[b * BLK : (b + 1) * BLK, lanes],
                k_ref[0:width, lanes],
                (((1,), (1,)), ((), ())),
                preferred_element_type=F32,
            )
            scores = scores * SCALE * jnp.exp(pair - peak)
            denoms.append(jnp.sum(scores, axis=1, keepdims=True))
            peaks.append(peak)
            numer_ref[b * BLK : (b + 1) * BLK, lanes] = jnp.dot(
                scores.astype(BF), v_ref[0:width, lanes], preferred_element_type=F32
            )
        lane = lax.broadcasted_iota(jnp.int32, (BLK, BLK), 1)
        aux = jnp.where(
            lane == 0,
            peaks[0],
            jnp.where(lane == 1, peaks[1], jnp.where(lane == 2, denoms[0], denoms[1])),
        )
        aux_ref[b * BLK : (b + 1) * BLK, :] = aux


def combine_kernel(
    gates_ref, q_ref, og_ref, gain_ref, numer_ref, aux_ref, s1, s2, s3, s4, full_ref
):
    gates = gates_ref[...]
    cum, totals = block_sums(gates)
    docs = gates[16:24, :]
    cum_cols = jnp.transpose(cum)
    doc_cols = jnp.transpose(docs)
    doc0 = docs[0:1, 0:1]
    smalls = []
    for s in (s1, s2, s3, s4):
        upper = s[256:272, :].astype(F32)
        lower = s[272:288, :].astype(F32)
        smalls.append(upper[0:8, :] + upper[8:16, :] + lower[0:8, :])
    states = []
    for h in range(HD):
        far = jnp.zeros((1, 1), F32)
        logs, valids = [], []
        for small in smalls:
            valid = small[6:7, 0:1] == doc0 + 1.0
            logs.append(jnp.where(valid, small[2 + h : 3 + h, 0:1] + far, NEG))
            valids.append(valid)
            far = far + small[4 + h : 5 + h, 0:1]
        stab = jnp.maximum(jnp.maximum(logs[0], logs[1]), jnp.maximum(logs[2], logs[3]))
        memory = jnp.zeros((DH, DH), F32)
        normer = jnp.zeros((1, DH), F32)
        for s, small, log, valid in zip((s1, s2, s3, s4), smalls, logs, valids):
            weight = jnp.where(valid, jnp.exp(log - stab), 0.0)
            memory = memory + weight * s[h * DH : (h + 1) * DH, :].astype(F32)
            normer = normer + weight * small[h : h + 1, :]
        states.append((memory.astype(BF), normer, stab))
    before = [jnp.zeros((1, 1), F32) for _ in range(HD)]
    for b in range(NB):
        rows = slice(b * BLK, (b + 1) * BLK)
        live = doc_cols[:, b : b + 1] == doc0
        aux = aux_ref[rows, :]
        squares = jnp.zeros((BLK, 1), F32)
        for h in range(HD):
            lanes = slice(h * DH, (h + 1) * DH)
            memory, normer, stab = states[h]
            r = h * NB + b
            carried = jnp.where(
                live & (stab > 0.5 * NEG), cum_cols[:, r : r + 1] + (before[h] + stab), NEG
            )
            peak = aux[:, h : h + 1]
            merged = jnp.maximum(peak, carried)
            own_w = jnp.exp(peak - merged)
            far_w = jnp.exp(carried - merged) * SCALE
            q_blk = q_ref[rows, lanes]
            numer = own_w * numer_ref[rows, lanes] + far_w * jnp.dot(
                q_blk, memory, preferred_element_type=F32
            )
            denom = own_w * aux[:, 2 + h : 3 + h] + far_w * jnp.sum(
                q_blk.astype(F32) * normer, axis=1, keepdims=True
            )
            cell = numer / jnp.maximum(jnp.abs(denom), 1.0)
            squares = squares + jnp.sum(cell * cell, axis=1, keepdims=True)
            gate = jax.nn.sigmoid(og_ref[rows, lanes].astype(F32))
            full_ref[rows, lanes] = (gate * cell * gain_ref[0:1, lanes].astype(F32)).astype(BF)
            before[h] = before[h] + totals[r]
        hi, mid, low = split3(squares)
        lane = lax.broadcasted_iota(jnp.int32, (BLK, BLK), 1)
        pieces = jnp.where(
            lane == 0,
            hi.astype(F32),
            jnp.where(lane == 1, mid.astype(F32), jnp.where(lane == 2, low.astype(F32), 0.0)),
        )
        full_ref[rows, 256:384] = pieces.astype(BF)


def project_kernel(at_ref, cells, resids, own_w, *refs):
    mine = refs[0:3]
    other = refs[3:6]
    first_ref, normed_ref, w_ref, g_ref, sem = refs[6:]
    core = at_ref[2]
    x = at_ref[3]

    def rows(rel, half):
        return pl.multiple_of(lax.rem(x + rel + 4, 4) * 256 + half * 128, 128)

    copies = [pltpu.make_async_copy(own_w, w_ref.at[pl.ds(rows(0, 0), 256)], sem)]
    for k in range(3):
        for part, half in ((mine[k], core), (other[k], 1 - core)):
            dst = w_ref.at[pl.ds(rows(REL[k + 1], half), 128)]
            copies.append(pltpu.make_async_copy(part, dst, sem))
    for copy in copies:
        copy.start()
    squares = jnp.zeros((OWN, 1), F32)
    for k in range(4):
        g_ref[:, k * 256 : (k + 1) * 256] = cells[k, :, 0:256]
        sent = cells[k, :, 256:384].astype(F32)
        squares = squares + (sent[:, 0:1] + sent[:, 1:2] + sent[:, 2:3])
    inverse = lax.rsqrt(squares / 1024.0 + EPS)
    for copy in copies:
        copy.wait()
    total = jnp.zeros((OWN, 1), F32)
    for a in range(4):
        cols = slice(a * 512, (a + 1) * 512)
        head = jnp.dot(g_ref[...], w_ref[:, cols], preferred_element_type=F32) * inverse
        first = (resids[a, 0:OWN, :].astype(F32) + head).astype(BF)
        first_ref[a] = first
        wide = first.astype(F32)
        total = total + jnp.sum(wide * wide, axis=1, keepdims=True)
    inverse = lax.rsqrt(total / float(D) + EPS)
    for a in range(4):
        cols = slice(a * 512, (a + 1) * 512)
        gain = resids[a, OWN : OWN + 16, :].astype(F32)[0:1, :]
        normed = (first_ref[a].astype(F32) * inverse * gain).astype(BF)
        for k in range(4):
            normed_ref[k, :, cols] = normed


def mixer_kernel(at_ref, x_ref, first_ref, weights, out_ref, up_ref, down_ref, sq_ref, sems):
    x = at_ref[3]

    def up_copy(f):
        return pltpu.make_async_copy(
            weights.at[:, pl.ds(0, 32), pl.ds(f * 512, 512)], up_ref.at[f], sems.at[f]
        )

    def down_copy(b):
        return pltpu.make_async_copy(
            weights.at[pl.ds(b * 16, 16), pl.ds(32, 32)], down_ref.at[b], sems.at[4 + b]
        )

    for f in range(4):
        up_copy(f).start()
    for b in range(4):
        down_copy(b).start()

    def up_step(f, carry):
        up_copy(f).wait()
        hidden = jnp.dot(
            x_ref[...].reshape(TOK, D),
            up_ref[f].reshape(D, 512),
            preferred_element_type=F32,
        )
        sq_ref[f] = jnp.square(jnp.maximum(hidden, 0.0)).astype(BF)
        return carry

    lax.fori_loop(0, 4, up_step, 0)

    def down_step(b, carry):
        down_copy(b).wait()
        part = jnp.zeros((TOK, 512), F32)
        for f in range(4):
            part = part + lax.dot_general(
                sq_ref[f],
                down_ref[b, :, :, f * 512 : (f + 1) * 512].reshape(512, 512),
                (((1,), (1,)), ((), ())),
                preferred_element_type=F32,
            )
        first = first_ref[b].astype(F32)
        for k in range(4):
            rows = slice(k * OWN, (k + 1) * OWN)
            piece = part[rows, :]
            out_ref[b, rows, :] = jnp.where(x == k, piece + first, piece).astype(BF)
        return carry

    lax.fori_loop(0, 4, down_step, 0)


def smem():
    return pl.BlockSpec(memory_space=pltpu.SMEM)


def vmem():
    return pl.BlockSpec(memory_space=pltpu.VMEM)


def hbm():
    return pl.BlockSpec(memory_space=pl.ANY)


def shape(*dims, dtype=BF):
    return jax.ShapeDtypeStruct(dims, dtype)


def call(body, name, specs, outs, scratch=(), flops=0):
    many = isinstance(outs, (list, tuple))
    return pl.pallas_call(
        body,
        name=name,
        in_specs=specs,
        out_specs=[vmem() for _ in outs] if many else vmem(),
        out_shape=outs,
        scratch_shapes=list(scratch),
        compiler_params=pltpu.CompilerParams(vmem_limit_bytes=56 * 1024 * 1024),
        cost_estimate=pl.CostEstimate(flops=flops, bytes_accessed=0, transcendentals=0),
    )


def exchange(value):
    return lax.all_to_all(value, "x", split_axis=0, concat_axis=0, tiled=True)


def local(
    queries,
    keys,
    values,
    output_gate_logits,
    input_gate_log,
    forget_gate_logits,
    extra_decay_log,
    document,
    residual,
    cell_norm_gain,
    output_weight,
    mixer_norm_gain,
    up_weight,
    down_weight,
):
    z, y, c, x = (lax.axis_index(a) for a in ("z", "y", "c", "x"))
    at = jnp.stack([z, y, c, x]).astype(jnp.int32)

    forget_log = jax.nn.log_sigmoid(forget_gate_logits) + extra_decay_log
    docs = document.astype(F32).reshape(NB, BLK)
    gates = jnp.concatenate(
        [input_gate_log.T.reshape(8, BLK), forget_log.T.reshape(8, BLK), docs, docs], axis=0
    )

    weights = lax.all_gather(jnp.concatenate([up_weight, down_weight.T], axis=0), SP)

    state = call(
        summary_kernel, "summary", [vmem()] * 3, shape(288, DH), flops=2 * 2 * 512 * 128 * 128
    )(gates, keys, values)
    states = [shift_sp(state, by) for by in (1, 2, 3, 4)]

    half = lax.dynamic_slice(output_weight, (c * 128, 0), (128, D))
    mine_w = [shift(half, "x", 1), shift(half, "x", -1), shift(half, "x", 2)]
    other_w = [shift(w, "c", 1) for w in mine_w]

    gain_rows = jnp.broadcast_to(mixer_norm_gain[None, None, :], (4, 16, 512))
    resids = exchange(jnp.concatenate([residual.reshape(4, OWN, 512), gain_rows], axis=1))

    numer, aux = call(
        local_kernel,
        "within",
        [vmem()] * 4,
        [shape(TOK, 256, dtype=F32), shape(TOK, BLK, dtype=F32)],
        flops=4 * 2 * 10 * 128**3,
    )(gates, queries, keys, values)
    cells = call(
        combine_kernel, "combine", [vmem()] * 10, shape(TOK, 384), flops=2 * 2 * 512 * 128 * 128
    )(gates, queries, output_gate_logits, cell_norm_gain[None, :], numer, aux, *states)

    first, normed = call(
        project_kernel,
        "project",
        [smem()] + [vmem()] * 2 + [hbm()] * 7,
        [shape(4, OWN, 512), shape(4, OWN, D)],
        [pltpu.VMEM((1024, D), BF), pltpu.VMEM((OWN, 1024), BF), pltpu.SemaphoreType.DMA],
        flops=2 * 128 * 1024 * 2048,
    )(at, exchange(cells.reshape(4, OWN, 384)), resids, output_weight, *mine_w, *other_w)

    parts = call(
        mixer_kernel,
        "mixer",
        [smem()] + [vmem()] * 2 + [hbm()],
        shape(4, TOK, 512),
        [
            pltpu.VMEM((4, 64, 32, 512), BF),
            pltpu.VMEM((4, 16, 32, FF), BF),
            pltpu.VMEM((4, TOK, 512), BF),
            pltpu.SemaphoreType.DMA((8,)),
        ],
        flops=4 * 512 * 2048 * 2048,
    )(at, exchange(normed), first, weights)
    return exchange(parts).astype(F32).sum(axis=0).astype(BF)


def solution(mesh):
    split = Mesh(mesh.devices.reshape(8, 4, 2, 4), ("z", "y", "c", "x"))
    return jax.shard_map(
        local,
        mesh=split,
        in_specs=(
            P(SP, "x"),
            P(SP, "x"),
            P(SP, "x"),
            P(SP, "x"),
            P(SP, "x"),
            P(SP, "x"),
            P(SP, "x"),
            P(SP),
            P(SP, "x"),
            P("x"),
            P("x", None),
            P("x"),
            P(SP, "x"),
            P("x", SP),
        ),
        out_specs=P(SP, "x"),
        check_vma=False,
    )
```

```python
import jax
import jax.numpy as jnp
from jax import lax
from jax.experimental import pallas as pl
from jax.experimental.pallas import tpu as pltpu
from jax.sharding import Mesh
from jax.sharding import PartitionSpec as P

NEG = -1e30
EPS = 1e-06
DH = 128
BLK = 128
NB = 4
HD = 2
TOK = 512
OWN = 128
D = 2048
FF = 2048
SCALE = DH ** (-0.5)
BF = jnp.bfloat16
F32 = jnp.float32
HIGH = lax.Precision.HIGHEST
SP = ("z", "y", "c")
REL = (0, -1, 1, 2)


def shift(value, axis, by):
    count = lax.axis_size(axis)
    return lax.ppermute(value, axis, [(i, (i + by) % count) for i in range(count)])


def shift_sp(value, by):
    return lax.ppermute(value, SP, [(i, i + by) for i in range(64 - by)])


def split3(value):
    hi = value.astype(BF)
    rest = value - hi.astype(F32)
    mid = rest.astype(BF)
    low = (rest - mid.astype(F32)).astype(BF)
    return hi, mid, low


def block_sums(gates):
    tri = (
        lax.broadcasted_iota(jnp.int32, (BLK, BLK), 0)
        <= lax.broadcasted_iota(jnp.int32, (BLK, BLK), 1)
    ).astype(F32)
    cum = jnp.dot(gates[8:16, :], tri, precision=HIGH, preferred_element_type=F32)
    totals = [cum[r : r + 1, BLK - 1 : BLK] for r in range(8)]
    return cum, totals


def summary_kernel(gates_ref, k_ref, v_ref, out_ref):
    gates = gates_ref[...]
    cum, totals = block_sums(gates)
    docs = gates[16:24, :]
    last_doc = docs[3:4, BLK - 1 : BLK]
    rows, stabs, sums = [], [], []
    for h in range(HD):
        keeps = []
        after = jnp.zeros((1, 1), F32)
        for b in reversed(range(NB)):
            r = h * NB + b
            keep = (totals[r] - cum[r : r + 1, :]) + after + gates[r : r + 1, :]
            keeps.append(jnp.where(docs[b : b + 1, :] == last_doc, keep, NEG))
            after = after + totals[r]
        keeps = keeps[::-1]
        stab = jnp.max(keeps[0], axis=1, keepdims=True)
        for keep in keeps[1:]:
            stab = jnp.maximum(stab, jnp.max(keep, axis=1, keepdims=True))
        rows += [jnp.exp(keep - stab) for keep in keeps]
        stabs.append(stab)
        sums.append(after)
    columns = jnp.transpose(jnp.concatenate(rows, axis=0))
    norms = []
    for h in range(HD):
        scaled = jnp.concatenate(
            [
                k_ref[b * BLK : (b + 1) * BLK, h * DH : (h + 1) * DH].astype(F32)
                * columns[:, h * NB + b : h * NB + b + 1]
                for b in range(NB)
            ],
            axis=0,
        )
        norms.append(jnp.sum(scaled, axis=0, keepdims=True))
        memory = lax.dot_general(
            scaled.astype(BF),
            v_ref[:, h * DH : (h + 1) * DH],
            (((0,), (0,)), ((), ())),
            preferred_element_type=F32,
        )
        out_ref[h * DH : (h + 1) * DH, :] = memory.astype(BF)
    wide = lambda a: jnp.broadcast_to(a, (1, BLK))
    small = jnp.concatenate(
        norms
        + [wide(a) for a in stabs]
        + [wide(a) for a in sums]
        + [wide(last_doc + 1.0), jnp.zeros((1, BLK), F32)],
        axis=0,
    )
    hi, mid, low = split3(small)
    pad = jnp.zeros((8, BLK), F32)
    out_ref[256:272, :] = jnp.concatenate([hi.astype(F32), mid.astype(F32)], axis=0).astype(BF)
    out_ref[272:288, :] = jnp.concatenate([low.astype(F32), pad], axis=0).astype(BF)


def local_kernel(gates_ref, q_ref, k_ref, v_ref, numer_ref, aux_ref):
    gates = gates_ref[...]
    cum, totals = block_sums(gates)
    docs = gates[16:24, :]
    cum_cols = jnp.transpose(cum)
    doc_cols = jnp.transpose(docs)
    for b in range(NB):
        width = (b + 1) * BLK
        row_at = lax.broadcasted_iota(jnp.int32, (BLK, width), 0) + b * BLK
        col_at = lax.broadcasted_iota(jnp.int32, (BLK, width), 1)
        doc_row = jnp.concatenate([docs[a : a + 1, :] for a in range(b + 1)], axis=1)
        mask = (doc_cols[:, b : b + 1] == doc_row) & (col_at <= row_at)
        peaks, denoms = [], []
        for h in range(HD):
            r = h * NB + b
            parts = [gates[r : r + 1, :] - cum[r : r + 1, :]]
            between = jnp.zeros((1, 1), F32)
            for a in reversed(range(b)):
                ra = h * NB + a
                parts.append((totals[ra] - cum[ra : ra + 1, :]) + between + gates[ra : ra + 1, :])
                between = between + totals[ra]
            source = jnp.concatenate(parts[::-1], axis=1)
            pair = jnp.where(mask, cum_cols[:, r : r + 1] + source, NEG)
            peak = jnp.max(pair, axis=1, keepdims=True)
            lanes = slice(h * DH, (h + 1) * DH)
            scores = lax.dot_general(
                q_ref[b * BLK : (b + 1) * BLK, lanes],
                k_ref[0:width, lanes],
                (((1,), (1,)), ((), ())),
                preferred_element_type=F32,
            )
            scores = scores * SCALE * jnp.exp(pair - peak)
            denoms.append(jnp.sum(scores, axis=1, keepdims=True))
            peaks.append(peak)
            numer_ref[b * BLK : (b + 1) * BLK, lanes] = jnp.dot(
                scores.astype(BF), v_ref[0:width, lanes], preferred_element_type=F32
            )
        lane = lax.broadcasted_iota(jnp.int32, (BLK, BLK), 1)
        aux = jnp.where(
            lane == 0,
            peaks[0],
            jnp.where(lane == 1, peaks[1], jnp.where(lane == 2, denoms[0], denoms[1])),
        )
        aux_ref[b * BLK : (b + 1) * BLK, :] = aux


def combine_kernel(
    gates_ref, q_ref, og_ref, gain_ref, numer_ref, aux_ref, s1, s2, s3, s4, full_ref
):
    gates = gates_ref[...]
    cum, totals = block_sums(gates)
    docs = gates[16:24, :]
    cum_cols = jnp.transpose(cum)
    doc_cols = jnp.transpose(docs)
    doc0 = docs[0:1, 0:1]
    smalls = []
    for s in (s1, s2, s3, s4):
        upper = s[256:272, :].astype(F32)
        lower = s[272:288, :].astype(F32)
        smalls.append(upper[0:8, :] + upper[8:16, :] + lower[0:8, :])
    states = []
    for h in range(HD):
        far = jnp.zeros((1, 1), F32)
        logs, valids = [], []
        for small in smalls:
            valid = small[6:7, 0:1] == doc0 + 1.0
            logs.append(jnp.where(valid, small[2 + h : 3 + h, 0:1] + far, NEG))
            valids.append(valid)
            far = far + small[4 + h : 5 + h, 0:1]
        stab = jnp.maximum(jnp.maximum(logs[0], logs[1]), jnp.maximum(logs[2], logs[3]))
        memory = jnp.zeros((DH, DH), F32)
        normer = jnp.zeros((1, DH), F32)
        for s, small, log, valid in zip((s1, s2, s3, s4), smalls, logs, valids):
            weight = jnp.where(valid, jnp.exp(log - stab), 0.0)
            memory = memory + weight * s[h * DH : (h + 1) * DH, :].astype(F32)
            normer = normer + weight * small[h : h + 1, :]
        states.append((memory.astype(BF), normer, stab))
    before = [jnp.zeros((1, 1), F32) for _ in range(HD)]
    for b in range(NB):
        rows = slice(b * BLK, (b + 1) * BLK)
        live = doc_cols[:, b : b + 1] == doc0
        aux = aux_ref[rows, :]
        squares = jnp.zeros((BLK, 1), F32)
        for h in range(HD):
            lanes = slice(h * DH, (h + 1) * DH)
            memory, normer, stab = states[h]
            r = h * NB + b
            carried = jnp.where(
                live & (stab > 0.5 * NEG), cum_cols[:, r : r + 1] + (before[h] + stab), NEG
            )
            peak = aux[:, h : h + 1]
            merged = jnp.maximum(peak, carried)
            own_w = jnp.exp(peak - merged)
            far_w = jnp.exp(carried - merged) * SCALE
            q_blk = q_ref[rows, lanes]
            numer = own_w * numer_ref[rows, lanes] + far_w * jnp.dot(
                q_blk, memory, preferred_element_type=F32
            )
            denom = own_w * aux[:, 2 + h : 3 + h] + far_w * jnp.sum(
                q_blk.astype(F32) * normer, axis=1, keepdims=True
            )
            cell = numer / jnp.maximum(jnp.abs(denom), 1.0)
            squares = squares + jnp.sum(cell * cell, axis=1, keepdims=True)
            gate = jax.nn.sigmoid(og_ref[rows, lanes].astype(F32))
            full_ref[rows, lanes] = (gate * cell * gain_ref[0:1, lanes].astype(F32)).astype(BF)
            before[h] = before[h] + totals[r]
        hi, mid, low = split3(squares)
        lane = lax.broadcasted_iota(jnp.int32, (BLK, BLK), 1)
        pieces = jnp.where(
            lane == 0,
            hi.astype(F32),
            jnp.where(lane == 1, mid.astype(F32), jnp.where(lane == 2, low.astype(F32), 0.0)),
        )
        full_ref[rows, 256:384] = pieces.astype(BF)


def project_kernel(at_ref, cells, resids, own_w, *refs):
    mine = refs[0:3]
    other = refs[3:6]
    first_ref, normed_ref, w_ref, g_ref, sem = refs[6:]
    core = at_ref[2]
    x = at_ref[3]

    def rows(rel, half):
        return pl.multiple_of(lax.rem(x + rel + 4, 4) * 256 + half * 128, 128)

    copies = [pltpu.make_async_copy(own_w, w_ref.at[pl.ds(rows(0, 0), 256)], sem)]
    for k in range(3):
        for part, half in ((mine[k], core), (other[k], 1 - core)):
            dst = w_ref.at[pl.ds(rows(REL[k + 1], half), 128)]
            copies.append(pltpu.make_async_copy(part, dst, sem))
    for copy in copies:
        copy.start()
    squares = jnp.zeros((OWN, 1), F32)
    for k in range(4):
        g_ref[:, k * 256 : (k + 1) * 256] = cells[k, :, 0:256]
        sent = cells[k, :, 256:384].astype(F32)
        squares = squares + (sent[:, 0:1] + sent[:, 1:2] + sent[:, 2:3])
    inverse = lax.rsqrt(squares / 1024.0 + EPS)
    for copy in copies:
        copy.wait()
    total = jnp.zeros((OWN, 1), F32)
    for a in range(4):
        cols = slice(a * 512, (a + 1) * 512)
        head = jnp.dot(g_ref[...], w_ref[:, cols], preferred_element_type=F32) * inverse
        first = (resids[a, 0:OWN, :].astype(F32) + head).astype(BF)
        first_ref[a] = first
        wide = first.astype(F32)
        total = total + jnp.sum(wide * wide, axis=1, keepdims=True)
    inverse = lax.rsqrt(total / float(D) + EPS)
    for a in range(4):
        cols = slice(a * 512, (a + 1) * 512)
        gain = resids[a, OWN : OWN + 16, :].astype(F32)[0:1, :]
        normed = (first_ref[a].astype(F32) * inverse * gain).astype(BF)
        for k in range(4):
            normed_ref[k, :, cols] = normed


def block_of(at_ref, rel):
    return lax.rem(at_ref[3] + rel + 4, 4)


def down_copy(weights, block, dst, sem):
    return pltpu.make_async_copy(weights.at[pl.ds(block * 16, 16), pl.ds(32, 32)], dst, sem)


def down_block(at_ref, sq_ref, first_ref, down, block):
    part = jnp.zeros((TOK, 512), F32)
    for f in range(4):
        part = part + lax.dot_general(
            sq_ref[f],
            down[:, :, f * 512 : (f + 1) * 512].reshape(512, 512),
            (((1,), (1,)), ((), ())),
            preferred_element_type=F32,
        )
    first = first_ref[block].astype(F32)
    pieces = []
    for k in range(4):
        piece = part[k * OWN : (k + 1) * OWN, :]
        pieces.append(jnp.where(at_ref[3] == k, piece + first, piece).astype(BF))
    return pieces


def up_kernel(
    at_ref, x_ref, first_ref, weights, sq_ref, low_ref, high_ref, up_ref, down_ref, sems
):
    def up_copy(f):
        return pltpu.make_async_copy(
            weights.at[:, pl.ds(0, 32), pl.ds(f * 512, 512)], up_ref.at[f], sems.at[f]
        )

    block = block_of(at_ref, 2)
    for f in range(4):
        up_copy(f).start()
    down_copy(weights, block, down_ref, sems.at[4]).start()

    def up_step(f, carry):
        up_copy(f).wait()
        hidden = jnp.dot(
            x_ref[...].reshape(TOK, D),
            up_ref[f].reshape(D, 512),
            preferred_element_type=F32,
        )
        sq_ref[f] = jnp.square(jnp.maximum(hidden, 0.0)).astype(BF)
        return carry

    lax.fori_loop(0, 4, up_step, 0)
    down_copy(weights, block, down_ref, sems.at[4]).wait()
    pieces = down_block(at_ref, sq_ref, first_ref, down_ref[...], block)
    for out, two in ((low_ref, pieces[:2]), (high_ref, pieces[2:])):
        for k in range(2):
            out[k * OWN : (k + 1) * OWN, :] = two[k]


def down_kernel(at_ref, sq_ref, first_ref, weights, *refs):
    outs, down_ref, sems = refs[:4], refs[4], refs[5]

    def copy(k):
        return down_copy(weights, block_of(at_ref, (1, -1)[k]), down_ref.at[k], sems.at[k])

    for k in range(2):
        copy(k).start()
    for k in range(2):
        copy(k).wait()
        pieces = down_block(at_ref, sq_ref, first_ref, down_ref[k], block_of(at_ref, (1, -1)[k]))
        for out, two in zip(outs[2 * k : 2 * k + 2], (pieces[:2], pieces[2:])):
            for i in range(2):
                out[i * OWN : (i + 1) * OWN, :] = two[i]


def last_kernel(at_ref, sq_ref, first_ref, weights, out_ref, down_ref, sem):
    block = block_of(at_ref, 0)
    copy = down_copy(weights, block, down_ref, sem)
    copy.start()
    copy.wait()
    for k, piece in enumerate(down_block(at_ref, sq_ref, first_ref, down_ref[...], block)):
        out_ref[k * OWN : (k + 1) * OWN, :] = piece


def smem():
    return pl.BlockSpec(memory_space=pltpu.SMEM)


def vmem():
    return pl.BlockSpec(memory_space=pltpu.VMEM)


def hbm():
    return pl.BlockSpec(memory_space=pl.ANY)


def shape(*dims, dtype=BF):
    return jax.ShapeDtypeStruct(dims, dtype)


def call(body, name, specs, outs, scratch=(), flops=0, mib=8):
    many = isinstance(outs, (list, tuple))
    return pl.pallas_call(
        body,
        name=name,
        in_specs=specs,
        out_specs=[vmem() for _ in outs] if many else vmem(),
        out_shape=outs,
        scratch_shapes=list(scratch),
        compiler_params=pltpu.CompilerParams(vmem_limit_bytes=mib * 1024 * 1024),
        cost_estimate=pl.CostEstimate(flops=flops, bytes_accessed=0, transcendentals=0),
    )


def exchange(value):
    return lax.all_to_all(value, "x", split_axis=0, concat_axis=0, tiled=True)


def local(
    queries,
    keys,
    values,
    output_gate_logits,
    input_gate_log,
    forget_gate_logits,
    extra_decay_log,
    document,
    residual,
    cell_norm_gain,
    output_weight,
    mixer_norm_gain,
    up_weight,
    down_weight,
):
    z, y, c, x = (lax.axis_index(a) for a in ("z", "y", "c", "x"))
    at = jnp.stack([z, y, c, x]).astype(jnp.int32)

    forget_log = jax.nn.log_sigmoid(forget_gate_logits) + extra_decay_log
    docs = document.astype(F32).reshape(NB, BLK)
    gates = jnp.concatenate(
        [input_gate_log.T.reshape(8, BLK), forget_log.T.reshape(8, BLK), docs, docs], axis=0
    )

    weights = lax.all_gather(jnp.concatenate([up_weight, down_weight.T], axis=0), SP)

    state = call(
        summary_kernel, "summary", [vmem()] * 3, shape(288, DH), flops=2 * 2 * 512 * 128 * 128
    )(gates, keys, values)
    states = [shift_sp(state, by) for by in (1, 2, 3, 4)]

    half = lax.dynamic_slice(output_weight, (c * 128, 0), (128, D))
    mine_w = [shift(half, "x", 1), shift(half, "x", -1), shift(half, "x", 2)]
    other_w = [shift(w, "c", 1) for w in mine_w]

    gain_rows = jnp.broadcast_to(mixer_norm_gain[None, None, :], (4, 16, 512))
    resids = exchange(jnp.concatenate([residual.reshape(4, OWN, 512), gain_rows], axis=1))

    numer, aux = call(
        local_kernel,
        "within",
        [vmem()] * 4,
        [shape(TOK, 256, dtype=F32), shape(TOK, BLK, dtype=F32)],
        flops=4 * 2 * 10 * 128**3,
    )(gates, queries, keys, values)
    cells = call(
        combine_kernel, "combine", [vmem()] * 10, shape(TOK, 384), flops=2 * 2 * 512 * 128 * 128
    )(gates, queries, output_gate_logits, cell_norm_gain[None, :], numer, aux, *states)

    first, normed = call(
        project_kernel,
        "project",
        [smem()] + [vmem()] * 2 + [hbm()] * 7,
        [shape(4, OWN, 512), shape(4, OWN, D)],
        [pltpu.VMEM((1024, D), BF), pltpu.VMEM((OWN, 1024), BF), pltpu.SemaphoreType.DMA],
        flops=2 * 128 * 1024 * 2048,
        mib=16,
    )(at, exchange(cells.reshape(4, OWN, 384)), resids, output_weight, *mine_w, *other_w)

    wide = exchange(normed)
    specs = [smem()] + [vmem()] * 2 + [hbm()]
    half_block = shape(TOK // 2, 512)
    down = pltpu.VMEM((16, 32, FF), BF)
    squared, far_low, far_high = call(
        up_kernel,
        "up",
        specs,
        [shape(4, TOK, 512), half_block, half_block],
        [pltpu.VMEM((4, 64, 32, 512), BF), down, pltpu.SemaphoreType.DMA((5,))],
        flops=2 * 512 * 2048 * 2560,
        mib=50,
    )(at, wide, first, weights)
    far_low, far_high = shift(far_low, "x", 1), shift(far_high, "x", -1)
    right_low, right_high, left_low, left_high = call(
        down_kernel,
        "down",
        specs,
        [half_block] * 4,
        [pltpu.VMEM((2, 16, 32, FF), BF), pltpu.SemaphoreType.DMA((2,))],
        flops=2 * 512 * 2048 * 1024,
        mib=50,
    )(at, squared, first, weights)
    from_left_high = shift(right_high, "x", 1)
    from_right_low = shift(left_low, "x", -1)
    add = lambda a, b: (a.astype(F32) + b.astype(F32)).astype(BF)
    from_left_low = shift(add(right_low, far_low), "x", 1)
    from_right_high = shift(add(left_high, far_high), "x", -1)
    own = call(
        last_kernel,
        "last",
        specs,
        shape(TOK, 512),
        [down, pltpu.SemaphoreType.DMA],
        flops=2 * 512 * 2048 * 512,
        mib=50,
    )(at, squared, first, weights)
    from_left = jnp.concatenate([from_left_low, from_left_high], axis=0)
    from_right = jnp.concatenate([from_right_low, from_right_high], axis=0)
    return (own.astype(F32) + from_left.astype(F32) + from_right.astype(F32)).astype(BF)


def solution(mesh):
    split = Mesh(mesh.devices.reshape(8, 4, 2, 4), ("z", "y", "c", "x"))
    return jax.shard_map(
        local,
        mesh=split,
        in_specs=(
            P(SP, "x"),
            P(SP, "x"),
            P(SP, "x"),
            P(SP, "x"),
            P(SP, "x"),
            P(SP, "x"),
            P(SP, "x"),
            P(SP),
            P(SP, "x"),
            P("x"),
            P("x", None),
            P("x"),
            P(SP, "x"),
            P("x", SP),
        ),
        out_specs=P(SP, "x"),
        check_vma=False,
    )
```

```python
import jax
import jax.numpy as jnp
from jax import lax
from jax.experimental import pallas as pl
from jax.experimental.pallas import tpu as pltpu
from jax.sharding import Mesh
from jax.sharding import PartitionSpec as P

NEG = -1e30
EPS = 1e-06
DH = 128
BLK = 128
NB = 4
HD = 2
TOK = 512
OWN = 128
D = 2048
FF = 2048
SCALE = DH ** (-0.5)
BF = jnp.bfloat16
F32 = jnp.float32
HIGH = lax.Precision.HIGHEST
SP = ("z", "y", "c")
REL = (0, -1, 1, 2)


def shift(value, axis, by):
    count = lax.axis_size(axis)
    return lax.ppermute(value, axis, [(i, (i + by) % count) for i in range(count)])


def after(value, *others):
    return lax.optimization_barrier((value, *others))[0]


def shift_sp(value, by):
    return lax.ppermute(value, SP, [(i, i + by) for i in range(64 - by)])


def split3(value):
    hi = value.astype(BF)
    rest = value - hi.astype(F32)
    mid = rest.astype(BF)
    low = (rest - mid.astype(F32)).astype(BF)
    return hi, mid, low


def block_sums(gates):
    tri = (
        lax.broadcasted_iota(jnp.int32, (BLK, BLK), 0)
        <= lax.broadcasted_iota(jnp.int32, (BLK, BLK), 1)
    ).astype(F32)
    cum = jnp.dot(gates[8:16, :], tri, precision=HIGH, preferred_element_type=F32)
    totals = [cum[r : r + 1, BLK - 1 : BLK] for r in range(8)]
    return cum, totals


def summary_kernel(gates_ref, k_ref, v_ref, out_ref):
    gates = gates_ref[...]
    cum, totals = block_sums(gates)
    docs = gates[16:24, :]
    last_doc = docs[3:4, BLK - 1 : BLK]
    rows, stabs, sums = [], [], []
    for h in range(HD):
        keeps = []
        after = jnp.zeros((1, 1), F32)
        for b in reversed(range(NB)):
            r = h * NB + b
            keep = (totals[r] - cum[r : r + 1, :]) + after + gates[r : r + 1, :]
            keeps.append(jnp.where(docs[b : b + 1, :] == last_doc, keep, NEG))
            after = after + totals[r]
        keeps = keeps[::-1]
        stab = jnp.max(keeps[0], axis=1, keepdims=True)
        for keep in keeps[1:]:
            stab = jnp.maximum(stab, jnp.max(keep, axis=1, keepdims=True))
        rows += [jnp.exp(keep - stab) for keep in keeps]
        stabs.append(stab)
        sums.append(after)
    columns = jnp.transpose(jnp.concatenate(rows, axis=0))
    norms = []
    for h in range(HD):
        scaled = jnp.concatenate(
            [
                k_ref[b * BLK : (b + 1) * BLK, h * DH : (h + 1) * DH].astype(F32)
                * columns[:, h * NB + b : h * NB + b + 1]
                for b in range(NB)
            ],
            axis=0,
        )
        norms.append(jnp.sum(scaled, axis=0, keepdims=True))
        memory = lax.dot_general(
            scaled.astype(BF),
            v_ref[:, h * DH : (h + 1) * DH],
            (((0,), (0,)), ((), ())),
            preferred_element_type=F32,
        )
        out_ref[h * DH : (h + 1) * DH, :] = memory.astype(BF)
    wide = lambda a: jnp.broadcast_to(a, (1, BLK))
    small = jnp.concatenate(
        norms
        + [wide(a) for a in stabs]
        + [wide(a) for a in sums]
        + [wide(last_doc + 1.0), jnp.zeros((1, BLK), F32)],
        axis=0,
    )
    hi, mid, low = split3(small)
    pad = jnp.zeros((8, BLK), F32)
    out_ref[256:272, :] = jnp.concatenate([hi.astype(F32), mid.astype(F32)], axis=0).astype(BF)
    out_ref[272:288, :] = jnp.concatenate([low.astype(F32), pad], axis=0).astype(BF)


def local_kernel(gates_ref, q_ref, k_ref, v_ref, numer_ref, aux_ref):
    gates = gates_ref[...]
    cum, totals = block_sums(gates)
    docs = gates[16:24, :]
    cum_cols = jnp.transpose(cum)
    doc_cols = jnp.transpose(docs)
    for b in range(NB):
        width = (b + 1) * BLK
        row_at = lax.broadcasted_iota(jnp.int32, (BLK, width), 0) + b * BLK
        col_at = lax.broadcasted_iota(jnp.int32, (BLK, width), 1)
        doc_row = jnp.concatenate([docs[a : a + 1, :] for a in range(b + 1)], axis=1)
        mask = (doc_cols[:, b : b + 1] == doc_row) & (col_at <= row_at)
        peaks, denoms = [], []
        for h in range(HD):
            r = h * NB + b
            parts = [gates[r : r + 1, :] - cum[r : r + 1, :]]
            between = jnp.zeros((1, 1), F32)
            for a in reversed(range(b)):
                ra = h * NB + a
                parts.append((totals[ra] - cum[ra : ra + 1, :]) + between + gates[ra : ra + 1, :])
                between = between + totals[ra]
            source = jnp.concatenate(parts[::-1], axis=1)
            pair = jnp.where(mask, cum_cols[:, r : r + 1] + source, NEG)
            peak = jnp.max(pair, axis=1, keepdims=True)
            lanes = slice(h * DH, (h + 1) * DH)
            scores = lax.dot_general(
                q_ref[b * BLK : (b + 1) * BLK, lanes],
                k_ref[0:width, lanes],
                (((1,), (1,)), ((), ())),
                preferred_element_type=F32,
            )
            scores = scores * SCALE * jnp.exp(pair - peak)
            denoms.append(jnp.sum(scores, axis=1, keepdims=True))
            peaks.append(peak)
            numer_ref[b * BLK : (b + 1) * BLK, lanes] = jnp.dot(
                scores.astype(BF), v_ref[0:width, lanes], preferred_element_type=F32
            )
        lane = lax.broadcasted_iota(jnp.int32, (BLK, BLK), 1)
        aux = jnp.where(
            lane == 0,
            peaks[0],
            jnp.where(lane == 1, peaks[1], jnp.where(lane == 2, denoms[0], denoms[1])),
        )
        aux_ref[b * BLK : (b + 1) * BLK, :] = aux


def combine_kernel(
    gates_ref, q_ref, og_ref, gain_ref, mixer_gain, numer_ref, aux_ref, s1, s2, s3, s4, full_ref
):
    gates = gates_ref[...]
    cum, totals = block_sums(gates)
    docs = gates[16:24, :]
    cum_cols = jnp.transpose(cum)
    doc_cols = jnp.transpose(docs)
    doc0 = docs[0:1, 0:1]
    smalls = []
    for s in (s1, s2, s3, s4):
        upper = s[256:272, :].astype(F32)
        lower = s[272:288, :].astype(F32)
        smalls.append(upper[0:8, :] + upper[8:16, :] + lower[0:8, :])
    states = []
    for h in range(HD):
        far = jnp.zeros((1, 1), F32)
        logs, valids = [], []
        for small in smalls:
            valid = small[6:7, 0:1] == doc0 + 1.0
            logs.append(jnp.where(valid, small[2 + h : 3 + h, 0:1] + far, NEG))
            valids.append(valid)
            far = far + small[4 + h : 5 + h, 0:1]
        stab = jnp.maximum(jnp.maximum(logs[0], logs[1]), jnp.maximum(logs[2], logs[3]))
        memory = jnp.zeros((DH, DH), F32)
        normer = jnp.zeros((1, DH), F32)
        for s, small, log, valid in zip((s1, s2, s3, s4), smalls, logs, valids):
            weight = jnp.where(valid, jnp.exp(log - stab), 0.0)
            memory = memory + weight * s[h * DH : (h + 1) * DH, :].astype(F32)
            normer = normer + weight * small[h : h + 1, :]
        states.append((memory.astype(BF), normer, stab))
    before = [jnp.zeros((1, 1), F32) for _ in range(HD)]
    lane = lax.broadcasted_iota(jnp.int32, (BLK, BLK), 1)
    table = jnp.zeros((BLK, BLK), F32)
    for b in range(NB):
        rows = slice(b * BLK, (b + 1) * BLK)
        live = doc_cols[:, b : b + 1] == doc0
        aux = aux_ref[rows, :]
        squares = jnp.zeros((BLK, 1), F32)
        for h in range(HD):
            lanes = slice(h * DH, (h + 1) * DH)
            memory, normer, stab = states[h]
            r = h * NB + b
            carried = jnp.where(
                live & (stab > 0.5 * NEG), cum_cols[:, r : r + 1] + (before[h] + stab), NEG
            )
            peak = aux[:, h : h + 1]
            merged = jnp.maximum(peak, carried)
            own_w = jnp.exp(peak - merged)
            far_w = jnp.exp(carried - merged) * SCALE
            q_blk = q_ref[rows, lanes]
            numer = own_w * numer_ref[rows, lanes] + far_w * jnp.dot(
                q_blk, memory, preferred_element_type=F32
            )
            denom = own_w * aux[:, 2 + h : 3 + h] + far_w * jnp.sum(
                q_blk.astype(F32) * normer, axis=1, keepdims=True
            )
            cell = numer / jnp.maximum(jnp.abs(denom), 1.0)
            squares = squares + jnp.sum(cell * cell, axis=1, keepdims=True)
            gate = jax.nn.sigmoid(og_ref[rows, lanes].astype(F32))
            full_ref[rows, lanes] = (gate * cell * gain_ref[0:1, lanes].astype(F32)).astype(BF)
            before[h] = before[h] + totals[r]
        table = jnp.where(lane == b, squares, table)
    hi, mid, low = (a.astype(F32) for a in split3(jnp.transpose(table)[0:8, :]))
    full_ref[TOK : TOK + 16, 0:128] = jnp.concatenate([hi, low], axis=0).astype(BF)
    gain = jnp.concatenate([mixer_gain[...].astype(F32), jnp.zeros((4, BLK), F32)], axis=0)
    full_ref[TOK : TOK + 16, 128:256] = jnp.concatenate([mid, gain], axis=0).astype(BF)


def block_of(at_ref, rel):
    return lax.rem(at_ref[3] + rel + 4, 4)


def project_kernel(at_ref, *refs):
    cells, resids, own_w = refs[0:4], refs[4:8], refs[8]
    mine, other = refs[9:12], refs[12:15]
    normed_ref, own_ref, w_ref, g_ref, r_ref, gain_ref, w_sem, r_sem = refs[15:]
    core = at_ref[2]
    weights = [pltpu.make_async_copy(own_w, w_ref.at[pl.ds(0, 256)], w_sem)]
    for k in range(3):
        for part, half in ((mine[k], core), (other[k], 1 - core)):
            start = pl.multiple_of((k + 1) * 256 + half * 128, 128)
            weights.append(pltpu.make_async_copy(part, w_ref.at[pl.ds(start, 128)], w_sem))
    rows = [
        pltpu.make_async_copy(part, r_ref.at[block_of(at_ref, rel)], r_sem)
        for part, rel in zip(resids, REL)
    ]
    for copy in weights + rows:
        copy.start()
    squares = jnp.zeros((8, BLK), F32)
    for k, rel in enumerate(REL):
        g_ref[:, k * 256 : (k + 1) * 256] = cells[k][0:TOK, :]
        left = cells[k][TOK : TOK + 16, 0:128].astype(F32)
        right = cells[k][TOK : TOK + 16, 128:256].astype(F32)
        squares = squares + (left[0:8, :] + right[0:8, :] + left[8:16, :])
        gain_ref[block_of(at_ref, rel)] = right[8:16, :]
    columns = jnp.transpose(lax.rsqrt(squares / 1024.0 + EPS))
    inverse = jnp.concatenate([columns[:, b : b + 1] for b in range(NB)], axis=0)
    for copy in weights + rows:
        copy.wait()

    def step(a, total):
        cols = pl.ds(pl.multiple_of(a * 512, 512), 512)
        head = jnp.dot(g_ref[...], w_ref[:, cols], preferred_element_type=F32) * inverse
        first = (r_ref[a].astype(F32) + head).astype(BF)
        r_ref[a] = first
        wide = first.astype(F32)
        return total + jnp.sum(wide * wide, axis=1, keepdims=True)

    total = lax.fori_loop(0, 4, step, jnp.zeros((TOK, 1), F32))
    own_ref[...] = r_ref[block_of(at_ref, 0)]
    inverse = lax.rsqrt(total / float(D) + EPS)
    for a in range(4):
        gain = jnp.concatenate([gain_ref[a, i : i + 1, :] for i in range(4)], axis=1)
        normed_ref[:, a * 512 : (a + 1) * 512] = (r_ref[a].astype(F32) * inverse * gain).astype(BF)


def pairs_kernel(own, p1, m1, a_ref, b_ref):
    a_ref[0:32, :] = own[...]
    a_ref[32:64, :] = p1[...]
    b_ref[0:32, :] = own[...]
    b_ref[32:64, :] = m1[...]


def ring_kernel(own, p1, m1, p4, a, b, out):
    for k, piece in enumerate((own, p1, m1, p4)):
        out[k * 32 : (k + 1) * 32, :] = piece[...]
    out[128:192, :] = a[...]
    out[192:256, :] = b[...]


def up_kernel(x_ref, weights, sq_ref, up_ref, sems):
    def up_copy(f):
        return pltpu.make_async_copy(weights.at[:, pl.ds(f * 512, 512)], up_ref.at[f], sems.at[f])

    for f in range(4):
        up_copy(f).start()

    def up_step(f, carry):
        up_copy(f).wait()
        hidden = jnp.dot(x_ref[...], up_ref[f], preferred_element_type=F32)
        cols = pl.ds(pl.multiple_of(f * 512, 512), 512)
        sq_ref[:, cols] = jnp.square(jnp.maximum(hidden, 0.0)).astype(BF)
        return carry

    lax.fori_loop(0, 4, up_step, 0)


def down_copies(at_ref, pieces, block, dst, sem):
    copies = []
    for i in range(2):
        dz = lax.rem(block * 2 + i - at_ref[0] + 8, 8)
        slot = jnp.int32(0)
        for at, key in enumerate((0, 7, 1, 4, 6, 5, 2, 3)):
            slot = jnp.where(dz == key, at, slot)
        for part, core in ((pieces[:4], at_ref[2]), (pieces[4:], 1 - at_ref[2])):
            for piece, dy in zip(part, REL):
                row = (i * 8 + lax.rem(at_ref[1] + dy + 4, 4) * 2 + core) * 32
                copies.append(
                    pltpu.make_async_copy(
                        piece.at[pl.ds(pl.multiple_of(slot * 32, 32), 32)],
                        dst.at[pl.ds(pl.multiple_of(row, 32), 32)],
                        sem,
                    )
                )
    return copies


def down_kernel(rels, split):
    def body(at_ref, sq_ref, *refs):
        pieces = refs[:8]
        outs, down_ref, part_ref, sems = refs[8:-3], refs[-3], refs[-2], refs[-1]

        def copies(k):
            rel = jnp.where(k == 0, rels[0], rels[-1])
            return down_copies(
                at_ref, pieces, block_of(at_ref, rel), down_ref.at[k], sems.at[k]
            )

        def start(k, carry):
            for copy in copies(k):
                copy.start()
            return carry

        def step(k, carry):
            for copy in copies(k):
                copy.wait()
            part_ref[k] = lax.dot_general(
                sq_ref[...],
                down_ref[k],
                (((1,), (1,)), ((), ())),
                preferred_element_type=F32,
            ).astype(BF)
            return carry

        lax.fori_loop(0, len(rels), start, 0)
        lax.fori_loop(0, len(rels), step, 0)
        for k in range(len(rels)):
            if split:
                outs[2 * k][...] = part_ref[k, 0 : TOK // 2, :]
                outs[2 * k + 1][...] = part_ref[k, TOK // 2 :, :]
            else:
                outs[k][...] = part_ref[k]

    return body


def smem():
    return pl.BlockSpec(memory_space=pltpu.SMEM)


def vmem():
    return pl.BlockSpec(memory_space=pltpu.VMEM)


def hbm():
    return pl.BlockSpec(memory_space=pl.ANY)


def shape(*dims, dtype=BF):
    return jax.ShapeDtypeStruct(dims, dtype)


def call(body, name, specs, outs, scratch=(), flops=0, mib=8):
    many = isinstance(outs, (list, tuple))
    return pl.pallas_call(
        body,
        name=name,
        in_specs=specs,
        out_specs=[vmem() for _ in outs] if many else vmem(),
        out_shape=outs,
        scratch_shapes=list(scratch),
        compiler_params=pltpu.CompilerParams(vmem_limit_bytes=mib * 1024 * 1024),
        cost_estimate=pl.CostEstimate(flops=flops, bytes_accessed=0, transcendentals=0),
    )


def local(
    queries,
    keys,
    values,
    output_gate_logits,
    input_gate_log,
    forget_gate_logits,
    extra_decay_log,
    document,
    residual,
    cell_norm_gain,
    output_weight,
    mixer_norm_gain,
    up_weight,
    down_weight,
):
    z, y, c, x = (lax.axis_index(a) for a in ("z", "y", "c", "x"))
    at = jnp.stack([z, y, c, x]).astype(jnp.int32)

    forget_log = jax.nn.log_sigmoid(forget_gate_logits) + extra_decay_log
    docs = document.astype(F32).reshape(NB, BLK)
    gates = jnp.concatenate(
        [input_gate_log.T.reshape(8, BLK), forget_log.T.reshape(8, BLK), docs, docs], axis=0
    )

    up_whole = lax.all_gather(up_weight, SP, axis=0, tiled=True)
    own = down_weight.T
    p1, m1, p4 = shift(own, "z", 1), shift(own, "z", -1), shift(own, "z", 4)

    state = call(
        summary_kernel, "summary", [vmem()] * 3, shape(288, DH), flops=2 * 2 * 512 * 128 * 128
    )(gates, keys, values)
    states = [shift_sp(state, by) for by in (1, 2, 3, 4)]

    half = lax.dynamic_slice(output_weight, (c * 128, 0), (128, D))
    mine_w = [shift(half, "x", 1), shift(half, "x", -1), shift(half, "x", 2)]

    resids = [residual, shift(residual, "x", 1), shift(residual, "x", -1), shift(residual, "x", 2)]

    pair = shape(64, FF)
    a2, b2 = call(pairs_kernel, "pairs", [vmem()] * 3, [pair, pair])(own, after(p1, gates), m1)
    a2, b2 = shift(a2, "z", 2), shift(b2, "z", -2)

    numer, aux = call(
        local_kernel,
        "within",
        [vmem()] * 4,
        [shape(TOK, 256, dtype=F32), shape(TOK, BLK, dtype=F32)],
        flops=4 * 2 * 10 * 128**3,
    )(gates, queries, keys, after(values, state))
    ring = call(ring_kernel, "ring", [vmem()] * 6, shape(256, FF))(
        own, p1, m1, p4, after(a2, aux), b2
    )
    downs = [ring, shift(ring, "y", 1), shift(ring, "y", -1), shift(ring, "y", 2)]
    cells = call(
        combine_kernel,
        "combine",
        [vmem()] * 11,
        shape(TOK + 16, 256),
        flops=2 * 2 * 512 * 128 * 128,
    )(
        gates,
        queries,
        output_gate_logits,
        cell_norm_gain[None, :],
        mixer_norm_gain.reshape(4, BLK),
        numer,
        aux,
        *states,
    )
    other_w = [shift(after(w, cells), "c", 1) for w in mine_w]
    cells = [cells, shift(cells, "x", 1), shift(cells, "x", -1), shift(cells, "x", 2)]

    normed, first = call(
        project_kernel,
        "project",
        [smem()] + [vmem()] * 4 + [hbm()] * 11,
        [shape(TOK, D), shape(TOK, 512)],
        [
            pltpu.VMEM((1024, D), BF),
            pltpu.VMEM((TOK, 1024), BF),
            pltpu.VMEM((4, TOK, 512), BF),
            pltpu.VMEM((4, 8, BLK), F32),
            pltpu.SemaphoreType.DMA,
            pltpu.SemaphoreType.DMA,
        ],
        flops=2 * 512 * 1024 * 2048,
        mib=24,
    )(at, *cells, *resids, output_weight, *mine_w, *other_w)

    downs += [shift(after(a, normed), "c", 1) for a in downs]
    squared = call(
        up_kernel,
        "up",
        [vmem(), hbm()],
        shape(TOK, FF),
        [pltpu.VMEM((4, D, 512), BF), pltpu.SemaphoreType.DMA((4,))],
        flops=2 * 512 * 2048 * 2048,
        mib=50,
    )(normed, up_whole)

    def down_call(name, rels, split):
        count = len(rels)
        return call(
            down_kernel(rels, split),
            name,
            [smem(), vmem()] + [hbm()] * 8,
            [shape(TOK // 2, 512)] * (2 * count) if split else [shape(TOK, 512)] * count,
            [
                pltpu.VMEM((count, 512, FF), BF),
                pltpu.VMEM((count, TOK, 512), BF),
                pltpu.SemaphoreType.DMA((count,)),
            ],
            flops=2 * 512 * 2048 * 512 * count,
            mib=24,
        )(at, squared, *downs)

    far_low, far_high = down_call("far", (2,), True)
    far_low, far_high = shift(far_low, "x", 1), shift(far_high, "x", -1)
    right_low, right_high, left_low, left_high = down_call("near", (1, -1), True)
    from_left_high = shift(right_high, "x", 1)
    from_right_low = shift(left_low, "x", -1)
    add = lambda a, b: (a.astype(F32) + b.astype(F32)).astype(BF)
    from_left_low = shift(add(right_low, far_low), "x", 1)
    from_right_high = shift(add(left_high, far_high), "x", -1)
    (own_term,) = down_call("last", (0,), False)
    from_left = jnp.concatenate([from_left_low, from_left_high], axis=0)
    from_right = jnp.concatenate([from_right_low, from_right_high], axis=0)
    terms = own_term.astype(F32) + from_left.astype(F32) + from_right.astype(F32)
    return (first.astype(F32) + terms).astype(BF)


def solution(mesh):
    split = Mesh(mesh.devices.reshape(8, 4, 2, 4), ("z", "y", "c", "x"))
    return jax.shard_map(
        local,
        mesh=split,
        in_specs=(
            P(SP, "x"),
            P(SP, "x"),
            P(SP, "x"),
            P(SP, "x"),
            P(SP, "x"),
            P(SP, "x"),
            P(SP, "x"),
            P(SP),
            P(SP, "x"),
            P("x"),
            P("x", None),
            P("x"),
            P(SP, "x"),
            P("x", SP),
        ),
        out_specs=P(SP, "x"),
        check_vma=False,
    )
```

```python
import jax
import jax.numpy as jnp
from jax import lax
from jax.experimental import pallas as pl
from jax.experimental.pallas import tpu as pltpu
from jax.sharding import Mesh
from jax.sharding import PartitionSpec as P

NEG = -1e30
EPS = 1e-06
DH = 128
BLK = 128
NB = 4
HD = 2
TOK = 512
D = 2048
FF = 2048
SCALE = DH ** (-0.5)
BF = jnp.bfloat16
F32 = jnp.float32
HIGH = lax.Precision.HIGHEST
SP = ("z", "y", "c")
REL = (0, -1, 1, 2)


def shift(value, axis, by):
    count = lax.axis_size(axis)
    return lax.ppermute(value, axis, [(i, (i + by) % count) for i in range(count)])


def shift_sp(value, by):
    return lax.ppermute(value, SP, [(i, i + by) for i in range(64 - by)])


def split3(value):
    hi = value.astype(BF)
    rest = value - hi.astype(F32)
    mid = rest.astype(BF)
    low = (rest - mid.astype(F32)).astype(BF)
    return hi, mid, low


def block_sums(gates):
    tri = (
        lax.broadcasted_iota(jnp.int32, (BLK, BLK), 0)
        <= lax.broadcasted_iota(jnp.int32, (BLK, BLK), 1)
    ).astype(F32)
    cum = jnp.dot(gates[8:16, :], tri, precision=HIGH, preferred_element_type=F32)
    totals = [cum[r : r + 1, BLK - 1 : BLK] for r in range(8)]
    return cum, totals


def summary_part(gates_ref, k_ref, v_ref, out_ref):
    gates = gates_ref[...]
    cum, totals = block_sums(gates)
    docs = gates[16:24, :]
    last_doc = docs[3:4, BLK - 1 : BLK]
    rows, stabs, sums = [], [], []
    for h in range(HD):
        keeps = []
        after = jnp.zeros((1, 1), F32)
        for b in reversed(range(NB)):
            r = h * NB + b
            keep = (totals[r] - cum[r : r + 1, :]) + after + gates[r : r + 1, :]
            keeps.append(jnp.where(docs[b : b + 1, :] == last_doc, keep, NEG))
            after = after + totals[r]
        keeps = keeps[::-1]
        stab = jnp.max(keeps[0], axis=1, keepdims=True)
        for keep in keeps[1:]:
            stab = jnp.maximum(stab, jnp.max(keep, axis=1, keepdims=True))
        rows += [jnp.exp(keep - stab) for keep in keeps]
        stabs.append(stab)
        sums.append(after)
    columns = jnp.transpose(jnp.concatenate(rows, axis=0))
    norms = []
    for h in range(HD):
        scaled = jnp.concatenate(
            [
                k_ref[b * BLK : (b + 1) * BLK, h * DH : (h + 1) * DH].astype(F32)
                * columns[:, h * NB + b : h * NB + b + 1]
                for b in range(NB)
            ],
            axis=0,
        )
        norms.append(jnp.sum(scaled, axis=0, keepdims=True))
        memory = lax.dot_general(
            scaled.astype(BF),
            v_ref[:, h * DH : (h + 1) * DH],
            (((0,), (0,)), ((), ())),
            preferred_element_type=F32,
        )
        out_ref[h * DH : (h + 1) * DH, :] = memory.astype(BF)
    wide = lambda a: jnp.broadcast_to(a, (1, BLK))
    small = jnp.concatenate(
        norms
        + [wide(a) for a in stabs]
        + [wide(a) for a in sums]
        + [wide(last_doc + 1.0), jnp.zeros((1, BLK), F32)],
        axis=0,
    )
    hi, mid, low = split3(small)
    pad = jnp.zeros((8, BLK), F32)
    out_ref[256:272, :] = jnp.concatenate([hi.astype(F32), mid.astype(F32)], axis=0).astype(BF)
    out_ref[272:288, :] = jnp.concatenate([low.astype(F32), pad], axis=0).astype(BF)


def cell_kernel(gates_ref, q_ref, k_ref, v_ref, state_ref, numer_ref, aux_ref):
    summary_part(gates_ref, k_ref, v_ref, state_ref)
    gates = gates_ref[...]
    cum, totals = block_sums(gates)
    docs = gates[16:24, :]
    cum_cols = jnp.transpose(cum)
    doc_cols = jnp.transpose(docs)
    for b in range(NB):
        width = (b + 1) * BLK
        row_at = lax.broadcasted_iota(jnp.int32, (BLK, width), 0) + b * BLK
        col_at = lax.broadcasted_iota(jnp.int32, (BLK, width), 1)
        doc_row = jnp.concatenate([docs[a : a + 1, :] for a in range(b + 1)], axis=1)
        mask = (doc_cols[:, b : b + 1] == doc_row) & (col_at <= row_at)
        peaks, denoms = [], []
        for h in range(HD):
            r = h * NB + b
            parts = [gates[r : r + 1, :] - cum[r : r + 1, :]]
            between = jnp.zeros((1, 1), F32)
            for a in reversed(range(b)):
                ra = h * NB + a
                parts.append((totals[ra] - cum[ra : ra + 1, :]) + between + gates[ra : ra + 1, :])
                between = between + totals[ra]
            source = jnp.concatenate(parts[::-1], axis=1)
            pair = jnp.where(mask, cum_cols[:, r : r + 1] + source, NEG)
            peak = jnp.max(pair, axis=1, keepdims=True)
            lanes = slice(h * DH, (h + 1) * DH)
            scores = lax.dot_general(
                q_ref[b * BLK : (b + 1) * BLK, lanes],
                k_ref[0:width, lanes],
                (((1,), (1,)), ((), ())),
                preferred_element_type=F32,
            )
            scores = scores * SCALE * jnp.exp(pair - peak)
            denoms.append(jnp.sum(scores, axis=1, keepdims=True))
            peaks.append(peak)
            numer_ref[b * BLK : (b + 1) * BLK, lanes] = jnp.dot(
                scores.astype(BF), v_ref[0:width, lanes], preferred_element_type=F32
            )
        lane = lax.broadcasted_iota(jnp.int32, (BLK, BLK), 1)
        aux = jnp.where(
            lane == 0,
            peaks[0],
            jnp.where(lane == 1, peaks[1], jnp.where(lane == 2, denoms[0], denoms[1])),
        )
        aux_ref[b * BLK : (b + 1) * BLK, :] = aux


def combine_kernel(
    gates_ref, q_ref, og_ref, gain_ref, mixer_gain, numer_ref, aux_ref, s1, s2, s3, s4, full_ref
):
    gates = gates_ref[...]
    cum, totals = block_sums(gates)
    docs = gates[16:24, :]
    cum_cols = jnp.transpose(cum)
    doc_cols = jnp.transpose(docs)
    doc0 = docs[0:1, 0:1]
    smalls = []
    for s in (s1, s2, s3, s4):
        upper = s[256:272, :].astype(F32)
        lower = s[272:288, :].astype(F32)
        smalls.append(upper[0:8, :] + upper[8:16, :] + lower[0:8, :])
    states = []
    for h in range(HD):
        far = jnp.zeros((1, 1), F32)
        logs, valids = [], []
        for small in smalls:
            valid = small[6:7, 0:1] == doc0 + 1.0
            logs.append(jnp.where(valid, small[2 + h : 3 + h, 0:1] + far, NEG))
            valids.append(valid)
            far = far + small[4 + h : 5 + h, 0:1]
        stab = jnp.maximum(jnp.maximum(logs[0], logs[1]), jnp.maximum(logs[2], logs[3]))
        memory = jnp.zeros((DH, DH), F32)
        normer = jnp.zeros((1, DH), F32)
        for s, small, log, valid in zip((s1, s2, s3, s4), smalls, logs, valids):
            weight = jnp.where(valid, jnp.exp(log - stab), 0.0)
            memory = memory + weight * s[h * DH : (h + 1) * DH, :].astype(F32)
            normer = normer + weight * small[h : h + 1, :]
        states.append((memory.astype(BF), normer, stab))
    before = [jnp.zeros((1, 1), F32) for _ in range(HD)]
    lane = lax.broadcasted_iota(jnp.int32, (BLK, BLK), 1)
    table = jnp.zeros((BLK, BLK), F32)
    for b in range(NB):
        rows = slice(b * BLK, (b + 1) * BLK)
        live = doc_cols[:, b : b + 1] == doc0
        aux = aux_ref[rows, :]
        squares = jnp.zeros((BLK, 1), F32)
        for h in range(HD):
            lanes = slice(h * DH, (h + 1) * DH)
            memory, normer, stab = states[h]
            r = h * NB + b
            carried = jnp.where(
                live & (stab > 0.5 * NEG), cum_cols[:, r : r + 1] + (before[h] + stab), NEG
            )
            peak = aux[:, h : h + 1]
            merged = jnp.maximum(peak, carried)
            own_w = jnp.exp(peak - merged)
            far_w = jnp.exp(carried - merged) * SCALE
            q_blk = q_ref[rows, lanes]
            numer = own_w * numer_ref[rows, lanes] + far_w * jnp.dot(
                q_blk, memory, preferred_element_type=F32
            )
            denom = own_w * aux[:, 2 + h : 3 + h] + far_w * jnp.sum(
                q_blk.astype(F32) * normer, axis=1, keepdims=True
            )
            cell = numer / jnp.maximum(jnp.abs(denom), 1.0)
            squares = squares + jnp.sum(cell * cell, axis=1, keepdims=True)
            gate = jax.nn.sigmoid(og_ref[rows, lanes].astype(F32))
            full_ref[rows, lanes] = (gate * cell * gain_ref[0:1, lanes].astype(F32)).astype(BF)
            before[h] = before[h] + totals[r]
        table = jnp.where(lane == b, squares, table)
    hi, mid, low = (a.astype(F32) for a in split3(jnp.transpose(table)[0:8, :]))
    full_ref[TOK : TOK + 16, 0:128] = jnp.concatenate([hi, low], axis=0).astype(BF)
    gain = jnp.concatenate([mixer_gain[...].astype(F32), jnp.zeros((4, BLK), F32)], axis=0)
    full_ref[TOK : TOK + 16, 128:256] = jnp.concatenate([mid, gain], axis=0).astype(BF)


def block_of(at_ref, rel):
    return lax.rem(at_ref[3] + rel + 4, 4)


def project_kernel(at_ref, *refs):
    cells, resids, own_w = refs[0:4], refs[4:8], refs[8]
    mine, other = refs[9:12], refs[12:15]
    normed_ref, own_ref, w_ref, g_ref, r_ref, gain_ref, w_sem, r_sem = refs[15:]
    core = at_ref[2]
    weights = [pltpu.make_async_copy(own_w, w_ref.at[pl.ds(0, 256)], w_sem)]
    for k in range(3):
        for part, half in ((mine[k], core), (other[k], 1 - core)):
            start = pl.multiple_of((k + 1) * 256 + half * 128, 128)
            weights.append(pltpu.make_async_copy(part, w_ref.at[pl.ds(start, 128)], w_sem))
    rows = [
        pltpu.make_async_copy(part, r_ref.at[block_of(at_ref, rel)], r_sem)
        for part, rel in zip(resids, REL)
    ]
    for copy in weights + rows:
        copy.start()
    squares = jnp.zeros((8, BLK), F32)
    for k, rel in enumerate(REL):
        g_ref[:, k * 256 : (k + 1) * 256] = cells[k][0:TOK, :]
        left = cells[k][TOK : TOK + 16, 0:128].astype(F32)
        right = cells[k][TOK : TOK + 16, 128:256].astype(F32)
        squares = squares + (left[0:8, :] + right[0:8, :] + left[8:16, :])
        gain_ref[block_of(at_ref, rel)] = right[8:16, :]
    columns = jnp.transpose(lax.rsqrt(squares / 1024.0 + EPS))
    inverse = jnp.concatenate([columns[:, b : b + 1] for b in range(NB)], axis=0)
    for copy in weights + rows:
        copy.wait()

    def step(a, total):
        cols = pl.ds(pl.multiple_of(a * 512, 512), 512)
        head = jnp.dot(g_ref[...], w_ref[:, cols], preferred_element_type=F32) * inverse
        first = (r_ref[a].astype(F32) + head).astype(BF)
        r_ref[a] = first
        wide = first.astype(F32)
        return total + jnp.sum(wide * wide, axis=1, keepdims=True)

    total = lax.fori_loop(0, 4, step, jnp.zeros((TOK, 1), F32))
    own_ref[...] = r_ref[block_of(at_ref, 0)]
    inverse = lax.rsqrt(total / float(D) + EPS)
    for a in range(4):
        gain = jnp.concatenate([gain_ref[a, i : i + 1, :] for i in range(4)], axis=1)
        normed_ref[:, a * 512 : (a + 1) * 512] = (r_ref[a].astype(F32) * inverse * gain).astype(BF)


def pairs_kernel(own, p1, m1, a_ref, b_ref):
    a_ref[0:32, :] = own[...]
    a_ref[32:64, :] = p1[...]
    b_ref[0:32, :] = own[...]
    b_ref[32:64, :] = m1[...]


def ring_kernel(own, p1, m1, p4, a, b, out):
    for k, piece in enumerate((own, p1, m1, p4)):
        out[k * 32 : (k + 1) * 32, :] = piece[...]
    out[128:192, :] = a[...]
    out[192:256, :] = b[...]


def shard_row(at_ref, dz, dy, core):
    z, y = lax.rem(at_ref[0] + dz + 8, 8), lax.rem(at_ref[1] + dy + 4, 4)
    return pl.multiple_of((z * 8 + y * 2 + core) * 32, 32)


def wait_all(dst, sem):
    pltpu.make_async_copy(dst, dst, sem).wait()


def up_kernel(at_ref, x_ref, *refs):
    ups, sq_ref, up_ref, sems = refs[:16], *refs[16:]
    cores = (at_ref[2], 1 - at_ref[2])

    def start(f, carry):
        cols = pl.ds(pl.multiple_of(f * 1024, 1024), 1024)
        for at, piece in enumerate(ups):
            dz = (0, -1, 1, -2, 2, -3, 3, 4)[at % 8]
            for k, dy in enumerate(REL):
                row = shard_row(at_ref, dz, dy, cores[at // 8])
                pltpu.make_async_copy(
                    piece.at[pl.ds(k * 32, 32), cols],
                    up_ref.at[f, pl.ds(row, 32)],
                    sems.at[f],
                ).start()
        return carry

    lax.fori_loop(0, 2, start, 0)

    def step(f, carry):
        @pl.when(lax.rem(f, 2) == 0)
        def _():
            wait_all(up_ref.at[f // 2], sems.at[f // 2])

        part = up_ref[f // 2, :, pl.ds(pl.multiple_of(lax.rem(f, 2) * 512, 512), 512)]
        hidden = jnp.dot(x_ref[...], part, preferred_element_type=F32)
        cols = pl.ds(pl.multiple_of(f * 512, 512), 512)
        sq_ref[:, cols] = jnp.square(jnp.maximum(hidden, 0.0)).astype(BF)
        return carry

    lax.fori_loop(0, 4, step, 0)


def down_term(sq_ref, down_ref):
    part = jnp.zeros((TOK, 512), F32)
    for f in range(4):
        cols = slice(f * 512, (f + 1) * 512)
        part = part + lax.dot_general(
            sq_ref[:, cols],
            down_ref[:, cols],
            (((1,), (1,)), ((), ())),
            preferred_element_type=F32,
        )
    return part.astype(BF)


def join_kernel(at_ref, *refs):
    pieces, outs = refs[:8], refs[8:12]
    cores = (at_ref[2], 1 - at_ref[2])
    for rel, dst in zip((2, 1, -1, 0), outs):
        block = block_of(at_ref, rel)

        def step(i, carry, dst=dst, block=block):
            dz = lax.rem(block * 2 + i - at_ref[0] + 8, 8)
            slot = jnp.int32(0)
            for at, key in enumerate((0, 7, 1, 4, 6, 5, 2, 3)):
                slot = jnp.where(dz == key, at, slot)
            src = pl.ds(pl.multiple_of(slot * 32, 32), 32)
            for at, piece in enumerate(pieces):
                y = lax.rem(at_ref[1] + REL[at % 4] + 4, 4)
                row = pl.multiple_of((i * 8 + y * 2 + cores[at // 4]) * 32, 32)
                dst[pl.ds(row, 32), :] = piece[src, :]
            return carry

        lax.fori_loop(0, 2, step, 0)


def down_kernel(sq_ref, *refs):
    count = len(refs) // 3
    for k, down_ref in enumerate(refs[:count]):
        part = down_term(sq_ref, down_ref)
        for i, out in enumerate(refs[count + 2 * k : count + 2 * k + 2]):
            out[...] = part[i * (TOK // 2) : (i + 1) * (TOK // 2), :]


def stack_kernel(*refs):
    out, at = refs[-1], 0
    for ref in refs[:-1]:
        out[at : at + ref.shape[0], :] = ref[...]
        at += ref.shape[0]


def smem():
    return pl.BlockSpec(memory_space=pltpu.SMEM)


def vmem():
    return pl.BlockSpec(memory_space=pltpu.VMEM)


def hbm():
    return pl.BlockSpec(memory_space=pl.ANY)


def shape(*dims, dtype=BF):
    return jax.ShapeDtypeStruct(dims, dtype)


def call(body, specs, outs, scratch=(), flops=0, mib=8):
    many = isinstance(outs, (list, tuple))
    return pl.pallas_call(
        body,
        in_specs=specs,
        out_specs=[vmem() for _ in outs] if many else vmem(),
        out_shape=outs,
        scratch_shapes=list(scratch),
        compiler_params=pltpu.CompilerParams(vmem_limit_bytes=mib * 1024 * 1024),
        cost_estimate=pl.CostEstimate(flops=flops, bytes_accessed=0, transcendentals=0),
    )


def local(
    queries,
    keys,
    values,
    output_gate_logits,
    input_gate_log,
    forget_gate_logits,
    extra_decay_log,
    document,
    residual,
    cell_norm_gain,
    output_weight,
    mixer_norm_gain,
    up_weight,
    down_weight,
):
    z, y, c, x = (lax.axis_index(a) for a in ("z", "y", "c", "x"))
    at = jnp.stack([z, y, c, x]).astype(jnp.int32)

    forget_log = jax.nn.log_sigmoid(forget_gate_logits) + extra_decay_log
    docs = document.astype(F32).reshape(NB, BLK)
    gates = jnp.concatenate(
        [input_gate_log.T.reshape(8, BLK), forget_log.T.reshape(8, BLK), docs, docs], axis=0
    )

    own = down_weight.T
    p1, m1 = shift(own, "z", 1), shift(own, "z", -1)
    up_y = [
        up_weight, shift(up_weight, "y", 1), shift(up_weight, "y", -1), shift(up_weight, "y", 2)
    ]

    state, numer, aux = call(
        cell_kernel,
        [vmem()] * 4,
        [shape(288, DH), shape(TOK, 256, dtype=F32), shape(TOK, BLK, dtype=F32)],
        flops=5 * 2 * 10 * 128**3,
    )(gates, queries, keys, values)
    states = [shift_sp(state, by) for by in (1, 2, 3, 4)]

    def to_all(value):
        return [shift(value, "x", by) for by in (1, -1, 2)]

    half = lax.dynamic_slice(output_weight, (c * 128, 0), (128, D))
    mine_w = to_all(half)
    other_w = [shift(w, "c", 1) for w in mine_w]
    resids = [residual, *to_all(residual)]

    pair = shape(64, FF)
    a2, b2 = call(pairs_kernel, [vmem()] * 3, [pair, pair])(own, p1, m1)
    a2, b2 = shift(a2, "z", 2), shift(b2, "z", -2)
    p4 = shift(own, "z", 4)
    ring = call(ring_kernel, [vmem()] * 6, shape(256, FF))(own, p1, m1, p4, a2, b2)
    downs = [ring, shift(ring, "y", 1), shift(ring, "y", -1), shift(ring, "y", 2)]
    downs += [shift(a, "c", 1) for a in downs]

    up_rows = call(stack_kernel, [vmem()] * 4, shape(128, FF))(*up_y)
    u1, d1 = shift(up_rows, "z", 1), shift(up_rows, "z", -1)
    u2, d2 = shift(u1, "z", 1), shift(d1, "z", -1)
    u3, d3 = shift(u2, "z", 1), shift(d2, "z", -1)
    ups = [up_rows, u1, d1, u2, d2, u3, d3, shift(u3, "z", 1)]
    ups += [shift(a, "c", 1) for a in ups]

    cells = call(
        combine_kernel, [vmem()] * 11, shape(TOK + 16, 256), flops=2 * 2 * 512 * 128 * 128
    )(
        gates,
        queries,
        output_gate_logits,
        cell_norm_gain[None, :],
        mixer_norm_gain.reshape(4, BLK),
        numer,
        aux,
        *states,
    )
    cells = [cells, *to_all(cells)]

    normed, first = call(
        project_kernel,
        [smem()] + [vmem()] * 4 + [hbm()] * 11,
        [shape(TOK, D), shape(TOK, 512)],
        [
            pltpu.VMEM((1024, D), BF),
            pltpu.VMEM((TOK, 1024), BF),
            pltpu.VMEM((4, TOK, 512), BF),
            pltpu.VMEM((4, 8, BLK), F32),
            pltpu.SemaphoreType.DMA,
            pltpu.SemaphoreType.DMA,
        ],
        flops=2 * 512 * 1024 * 2048,
        mib=24,
    )(at, *cells, *resids, output_weight, *mine_w, *other_w)

    far_down, right_down, left_down, own_down = call(
        join_kernel, [smem()] + [vmem()] * 8, [shape(512, FF)] * 4, flops=2**30, mib=18
    )(at, *downs)
    squared = call(
        up_kernel,
        [smem(), vmem()] + [hbm()] * 16,
        shape(TOK, FF),
        [pltpu.VMEM((2, D, 1024), BF), pltpu.SemaphoreType.DMA((2,))],
        flops=2 * 512 * 2048 * 2048,
        mib=14,
    )(at, normed, *ups)

    def down_call(*blocks):
        return call(
            down_kernel,
            [vmem()] * (1 + len(blocks)),
            [shape(TOK // 2, 512)] * (2 * len(blocks)),
            flops=2 * 512 * 2048 * 512 * len(blocks),
            mib=12,
        )(squared, *blocks)

    far_low, far_high = down_call(far_down)
    far_low, far_high = shift(far_low, "x", 1), shift(far_high, "x", -1)
    right_low, right_high, left_low, left_high = down_call(right_down, left_down)
    from_left_high = shift(right_high, "x", 1)
    from_right_low = shift(left_low, "x", -1)
    add = lambda a, b: (a.astype(F32) + b.astype(F32)).astype(BF)
    from_left_low = shift(add(right_low, far_low), "x", 1)
    from_right_high = shift(add(left_high, far_high), "x", -1)
    own_low, own_high = down_call(own_down)
    own_term = jnp.concatenate([own_low, own_high], axis=0)
    from_left = jnp.concatenate([from_left_low, from_left_high], axis=0)
    from_right = jnp.concatenate([from_right_low, from_right_high], axis=0)
    terms = own_term.astype(F32) + from_left.astype(F32) + from_right.astype(F32)
    return (first.astype(F32) + terms).astype(BF)


def solution(mesh):
    split = Mesh(mesh.devices.reshape(8, 4, 2, 4), ("z", "y", "c", "x"))

    return jax.shard_map(
        local,
        mesh=split,
        in_specs=(
            P(SP, "x"),
            P(SP, "x"),
            P(SP, "x"),
            P(SP, "x"),
            P(SP, "x"),
            P(SP, "x"),
            P(SP, "x"),
            P(SP),
            P(SP, "x"),
            P("x"),
            P("x", None),
            P("x"),
            P(SP, "x"),
            P("x", SP),
        ),
        out_specs=P(SP, "x"),
        check_vma=False,
    )
```

```python
import jax
import jax.numpy as jnp
from jax import lax
from jax.experimental import pallas as pl
from jax.experimental.pallas import tpu as pltpu
from jax.sharding import Mesh
from jax.sharding import PartitionSpec as P

NEG = -1e30
EPS = 1e-06
DH = 128
BLK = 128
NB = 4
HD = 2
TOK = 512
D = 2048
FF = 2048
SCALE = DH ** (-0.5)
BF = jnp.bfloat16
F32 = jnp.float32
HIGH = lax.Precision.HIGHEST
SP = ("z", "y", "c")
REL = (0, -1, 1, 2)


def shift(value, axis, by):
    count = lax.axis_size(axis)
    return lax.ppermute(value, axis, [(i, (i + by) % count) for i in range(count)])


def shift_sp(value, by):
    return lax.ppermute(value, SP, [(i, i + by) for i in range(64 - by)])


def split3(value):
    hi = value.astype(BF)
    rest = value - hi.astype(F32)
    mid = rest.astype(BF)
    low = (rest - mid.astype(F32)).astype(BF)
    return hi, mid, low


def block_sums(gates):
    tri = (
        lax.broadcasted_iota(jnp.int32, (BLK, BLK), 0)
        <= lax.broadcasted_iota(jnp.int32, (BLK, BLK), 1)
    ).astype(F32)
    cum = jnp.dot(gates[8:16, :], tri, precision=HIGH, preferred_element_type=F32)
    totals = [cum[r : r + 1, BLK - 1 : BLK] for r in range(8)]
    return cum, totals


def summary_part(gates_ref, k_ref, v_ref, out_ref):
    gates = gates_ref[...]
    cum, totals = block_sums(gates)
    docs = gates[16:24, :]
    last_doc = docs[3:4, BLK - 1 : BLK]
    rows, stabs, sums = [], [], []
    for h in range(HD):
        keeps = []
        after = jnp.zeros((1, 1), F32)
        for b in reversed(range(NB)):
            r = h * NB + b
            keep = (totals[r] - cum[r : r + 1, :]) + after + gates[r : r + 1, :]
            keeps.append(jnp.where(docs[b : b + 1, :] == last_doc, keep, NEG))
            after = after + totals[r]
        keeps = keeps[::-1]
        stab = jnp.max(keeps[0], axis=1, keepdims=True)
        for keep in keeps[1:]:
            stab = jnp.maximum(stab, jnp.max(keep, axis=1, keepdims=True))
        rows += [jnp.exp(keep - stab) for keep in keeps]
        stabs.append(stab)
        sums.append(after)
    columns = jnp.transpose(jnp.concatenate(rows, axis=0))
    norms = []
    for h in range(HD):
        scaled = jnp.concatenate(
            [
                k_ref[b * BLK : (b + 1) * BLK, h * DH : (h + 1) * DH].astype(F32)
                * columns[:, h * NB + b : h * NB + b + 1]
                for b in range(NB)
            ],
            axis=0,
        )
        norms.append(jnp.sum(scaled, axis=0, keepdims=True))
        memory = lax.dot_general(
            scaled.astype(BF),
            v_ref[:, h * DH : (h + 1) * DH],
            (((0,), (0,)), ((), ())),
            preferred_element_type=F32,
        )
        out_ref[h * DH : (h + 1) * DH, :] = memory.astype(BF)
    wide = lambda a: jnp.broadcast_to(a, (1, BLK))
    small = jnp.concatenate(
        norms
        + [wide(a) for a in stabs]
        + [wide(a) for a in sums]
        + [wide(last_doc + 1.0), jnp.zeros((1, BLK), F32)],
        axis=0,
    )
    hi, mid, low = split3(small)
    pad = jnp.zeros((8, BLK), F32)
    out_ref[256:272, :] = jnp.concatenate([hi.astype(F32), mid.astype(F32)], axis=0).astype(BF)
    out_ref[272:288, :] = jnp.concatenate([low.astype(F32), pad], axis=0).astype(BF)


def cell_kernel(gates_ref, q_ref, k_ref, v_ref, state_ref, numer_ref, aux_ref):
    summary_part(gates_ref, k_ref, v_ref, state_ref)
    gates = gates_ref[...]
    cum, totals = block_sums(gates)
    docs = gates[16:24, :]
    cum_cols = jnp.transpose(cum)
    doc_cols = jnp.transpose(docs)
    for b in range(NB):
        width = (b + 1) * BLK
        row_at = lax.broadcasted_iota(jnp.int32, (BLK, width), 0) + b * BLK
        col_at = lax.broadcasted_iota(jnp.int32, (BLK, width), 1)
        doc_row = jnp.concatenate([docs[a : a + 1, :] for a in range(b + 1)], axis=1)
        mask = (doc_cols[:, b : b + 1] == doc_row) & (col_at <= row_at)
        peaks, denoms = [], []
        for h in range(HD):
            r = h * NB + b
            parts = [gates[r : r + 1, :] - cum[r : r + 1, :]]
            between = jnp.zeros((1, 1), F32)
            for a in reversed(range(b)):
                ra = h * NB + a
                parts.append((totals[ra] - cum[ra : ra + 1, :]) + between + gates[ra : ra + 1, :])
                between = between + totals[ra]
            source = jnp.concatenate(parts[::-1], axis=1)
            pair = jnp.where(mask, cum_cols[:, r : r + 1] + source, NEG)
            peak = jnp.max(pair, axis=1, keepdims=True)
            lanes = slice(h * DH, (h + 1) * DH)
            scores = lax.dot_general(
                q_ref[b * BLK : (b + 1) * BLK, lanes],
                k_ref[0:width, lanes],
                (((1,), (1,)), ((), ())),
                preferred_element_type=F32,
            )
            scores = scores * SCALE * jnp.exp(pair - peak)
            denoms.append(jnp.sum(scores, axis=1, keepdims=True))
            peaks.append(peak)
            numer_ref[b * BLK : (b + 1) * BLK, lanes] = jnp.dot(
                scores.astype(BF), v_ref[0:width, lanes], preferred_element_type=F32
            )
        lane = lax.broadcasted_iota(jnp.int32, (BLK, BLK), 1)
        aux = jnp.where(
            lane == 0,
            peaks[0],
            jnp.where(lane == 1, peaks[1], jnp.where(lane == 2, denoms[0], denoms[1])),
        )
        aux_ref[b * BLK : (b + 1) * BLK, :] = aux


def combine_kernel(
    gates_ref, q_ref, og_ref, gain_ref, mixer_gain, numer_ref, aux_ref, s1, s2, s3, s4, full_ref, far_ref
):
    gates = gates_ref[...]
    cum, totals = block_sums(gates)
    docs = gates[16:24, :]
    cum_cols = jnp.transpose(cum)
    doc_cols = jnp.transpose(docs)
    doc0 = docs[0:1, 0:1]
    smalls = []
    for s in (s1, s2, s3, s4):
        upper = s[256:272, :].astype(F32)
        lower = s[272:288, :].astype(F32)
        smalls.append(upper[0:8, :] + upper[8:16, :] + lower[0:8, :])
    states = []
    for h in range(HD):
        far = jnp.zeros((1, 1), F32)
        logs, valids = [], []
        for small in smalls:
            valid = small[6:7, 0:1] == doc0 + 1.0
            logs.append(jnp.where(valid, small[2 + h : 3 + h, 0:1] + far, NEG))
            valids.append(valid)
            far = far + small[4 + h : 5 + h, 0:1]
        stab = jnp.maximum(jnp.maximum(logs[0], logs[1]), jnp.maximum(logs[2], logs[3]))
        memory = jnp.zeros((DH, DH), F32)
        normer = jnp.zeros((1, DH), F32)
        for s, small, log, valid in zip((s1, s2, s3, s4), smalls, logs, valids):
            weight = jnp.where(valid, jnp.exp(log - stab), 0.0)
            memory = memory + weight * s[h * DH : (h + 1) * DH, :].astype(F32)
            normer = normer + weight * small[h : h + 1, :]
        states.append((memory.astype(BF), normer, stab))
    before = [jnp.zeros((1, 1), F32) for _ in range(HD)]
    lane = lax.broadcasted_iota(jnp.int32, (BLK, BLK), 1)
    for b in range(NB):
        live = doc_cols[:, b : b + 1] == doc0
        far = []
        for h in range(HD):
            r = h * NB + b
            stab = states[h][2]
            log = cum_cols[:, r : r + 1] + (before[h] + stab)
            far.append(jnp.where(live & (stab > 0.5 * NEG), log, NEG))
            before[h] = before[h] + totals[r]
        far_ref[b] = jnp.where(lane == 0, far[0], far[1])

    def step(b, table):
        rows = pl.ds(pl.multiple_of(b * BLK, BLK), BLK)
        aux = aux_ref[rows, :]
        logs = far_ref[b]
        squares = jnp.zeros((BLK, 1), F32)
        for h in range(HD):
            lanes = slice(h * DH, (h + 1) * DH)
            memory, normer, _ = states[h]
            carried = logs[:, h : h + 1]
            peak = aux[:, h : h + 1]
            merged = jnp.maximum(peak, carried)
            own_w = jnp.exp(peak - merged)
            far_w = jnp.exp(carried - merged) * SCALE
            q_blk = q_ref[rows, lanes]
            numer = own_w * numer_ref[rows, lanes] + far_w * jnp.dot(
                q_blk, memory, preferred_element_type=F32
            )
            denom = own_w * aux[:, 2 + h : 3 + h] + far_w * jnp.sum(
                q_blk.astype(F32) * normer, axis=1, keepdims=True
            )
            cell = numer / jnp.maximum(jnp.abs(denom), 1.0)
            squares = squares + jnp.sum(cell * cell, axis=1, keepdims=True)
            gate = jax.nn.sigmoid(og_ref[rows, lanes].astype(F32))
            full_ref[rows, lanes] = (gate * cell * gain_ref[0:1, lanes].astype(F32)).astype(BF)
        return jnp.where(lane == b, squares, table)

    table = lax.fori_loop(0, NB, step, jnp.zeros((BLK, BLK), F32))
    hi, mid, low = (a.astype(F32) for a in split3(jnp.transpose(table)[0:8, :]))
    full_ref[TOK : TOK + 16, 0:128] = jnp.concatenate([hi, low], axis=0).astype(BF)
    gain = jnp.concatenate([mixer_gain[...].astype(F32), jnp.zeros((4, BLK), F32)], axis=0)
    full_ref[TOK : TOK + 16, 128:256] = jnp.concatenate([mid, gain], axis=0).astype(BF)


def block_of(at_ref, rel):
    return lax.rem(at_ref[3] + rel + 4, 4)


def project_kernel(at_ref, *refs):
    cells, own_resid, own_w = refs[0:4], refs[4], refs[5]
    packs, other = refs[6:9], refs[9]
    normed_ref, own_ref, w_ref, g_ref, r_ref, gain_ref, w_sem, r_sem = refs[10:]
    core = at_ref[2]
    weights = [pltpu.make_async_copy(own_w, w_ref.at[pl.ds(0, 256)], w_sem)]
    rows = [pltpu.make_async_copy(own_resid, r_ref.at[block_of(at_ref, 0)], r_sem)]
    for k, pack in enumerate(packs):
        parts = ((pack, 0, core), (other, k * 128, 1 - core))
        for part, at, half in parts:
            start = pl.multiple_of((k + 1) * 256 + half * 128, 128)
            weights.append(
                pltpu.make_async_copy(
                    part.at[pl.ds(at, 128)], w_ref.at[pl.ds(start, 128)], w_sem
                )
            )
        for i in range(4):
            rows.append(
                pltpu.make_async_copy(
                    pack.at[pl.ds(128, 128), pl.ds(i * 512, 512)],
                    r_ref.at[block_of(at_ref, REL[k + 1]), pl.ds(i * 128, 128)],
                    r_sem,
                )
            )
    for copy in weights + rows:
        copy.start()
    squares = jnp.zeros((8, BLK), F32)
    for k, rel in enumerate(REL):
        g_ref[:, k * 256 : (k + 1) * 256] = cells[k][0:TOK, :]
        left = cells[k][TOK : TOK + 16, 0:128].astype(F32)
        right = cells[k][TOK : TOK + 16, 128:256].astype(F32)
        squares = squares + (left[0:8, :] + right[0:8, :] + left[8:16, :])
        gain_ref[block_of(at_ref, rel)] = right[8:16, :]
    columns = jnp.transpose(lax.rsqrt(squares / 1024.0 + EPS))
    inverse = jnp.concatenate([columns[:, b : b + 1] for b in range(NB)], axis=0)
    for copy in weights + rows:
        copy.wait()

    def step(a, total):
        cols = pl.ds(pl.multiple_of(a * 512, 512), 512)
        head = jnp.dot(g_ref[...], w_ref[:, cols], preferred_element_type=F32) * inverse
        first = (r_ref[a].astype(F32) + head).astype(BF)
        r_ref[a] = first
        wide = first.astype(F32)
        return total + jnp.sum(wide * wide, axis=1, keepdims=True)

    total = lax.fori_loop(0, 4, step, jnp.zeros((TOK, 1), F32))
    own_ref[...] = r_ref[block_of(at_ref, 0)]
    inverse = lax.rsqrt(total / float(D) + EPS)

    def scale(a, carry):
        gain = gain_ref[a]
        gain = jnp.concatenate([gain[i : i + 1, :] for i in range(4)], axis=1)
        cols = pl.ds(pl.multiple_of(a * 512, 512), 512)
        normed_ref[:, cols] = (r_ref[a].astype(F32) * inverse * gain).astype(BF)
        return carry

    lax.fori_loop(0, 4, scale, 0)


def pack_kernel(at_ref, weight_ref, resid_ref, out_ref):
    start = pl.multiple_of(at_ref[2] * 128, 128)
    out_ref[0:128, :] = weight_ref[pl.ds(start, 128), :]
    for i in range(4):
        out_ref[128:256, i * 512 : (i + 1) * 512] = resid_ref[i * 128 : (i + 1) * 128, :]


def heads_kernel(a, b, c, out_ref):
    for k, ref in enumerate((a, b, c)):
        out_ref[k * 128 : (k + 1) * 128, :] = ref[0:128, :]


def pairs_kernel(own, p1, m1, a_ref, b_ref):
    a_ref[0:32, :] = own[...]
    a_ref[32:64, :] = p1[...]
    b_ref[0:32, :] = own[...]
    b_ref[32:64, :] = m1[...]


def ring_kernel(own, p1, m1, p4, a, b, out):
    for k, piece in enumerate((own, p1, m1, p4)):
        out[k * 32 : (k + 1) * 32, :] = piece[...]
    out[128:192, :] = a[...]
    out[192:256, :] = b[...]


def shard_row(at_ref, dz, dy, core):
    z, y = lax.rem(at_ref[0] + dz + 8, 8), lax.rem(at_ref[1] + dy + 4, 4)
    return pl.multiple_of((z * 8 + y * 2 + core) * 32, 32)


def wait_all(dst, sem):
    pltpu.make_async_copy(dst, dst, sem).wait()


def up_kernel(at_ref, x_ref, *refs):
    own, other = refs[:8], refs[8:11]
    sq_ref, up_ref, sems = refs[11:]
    cores = (at_ref[2], 1 - at_ref[2])

    def start(f, carry):
        cols = pl.ds(pl.multiple_of(f * 1024, 1024), 1024)
        pieces = [(piece, 0) for piece in own]
        pieces += [(other[n], 128 * k) for n, count in enumerate((5, 2, 1)) for k in range(count)]
        for n, (piece, at) in enumerate(pieces):
            dz = (0, -1, 1, -2, 2, -3, 3, 4)[n % 8]
            for k, dy in enumerate(REL):
                row = shard_row(at_ref, dz, dy, cores[n // 8])
                pltpu.make_async_copy(
                    piece.at[pl.ds(at + k * 32, 32), cols],
                    up_ref.at[f, pl.ds(row, 32)],
                    sems.at[f],
                ).start()
        return carry

    lax.fori_loop(0, 2, start, 0)

    def step(f, carry):
        @pl.when(lax.rem(f, 2) == 0)
        def _():
            wait_all(up_ref.at[f // 2], sems.at[f // 2])

        part = up_ref[f // 2, :, pl.ds(pl.multiple_of(lax.rem(f, 2) * 512, 512), 512)]
        hidden = jnp.dot(x_ref[...], part, preferred_element_type=F32)
        cols = pl.ds(pl.multiple_of(f * 512, 512), 512)
        sq_ref[:, cols] = jnp.square(jnp.maximum(hidden, 0.0)).astype(BF)
        return carry

    lax.fori_loop(0, 4, step, 0)


def down_term(sq_ref, down_ref):
    part = jnp.zeros((TOK, 512), F32)
    for f in range(4):
        cols = slice(f * 512, (f + 1) * 512)
        part = part + lax.dot_general(
            sq_ref[:, cols],
            down_ref[:, cols],
            (((1,), (1,)), ((), ())),
            preferred_element_type=F32,
        )
    return part.astype(BF)


def join_kernel(at_ref, *refs):
    far_ref, near_ref, last_ref = refs[7:]
    own, (other0, other1, other3) = refs[:4], refs[4:7]
    pieces = [(piece, 0) for piece in own]
    pieces += [(other0, 0), (other1, 0), (other1, 256), (other3, 0)]
    cores = (at_ref[2], 1 - at_ref[2])
    outs = (far_ref, near_ref.at[0], near_ref.at[1], last_ref)
    for rel, dst in zip((2, 1, -1, 0), outs):
        block = block_of(at_ref, rel)

        def step(i, carry, dst=dst, block=block):
            dz = lax.rem(block * 2 + i - at_ref[0] + 8, 8)
            slot = jnp.int32(0)
            for at, key in enumerate((0, 7, 1, 4, 6, 5, 2, 3)):
                slot = jnp.where(dz == key, at, slot)
            for n, (piece, at) in enumerate(pieces):
                y = lax.rem(at_ref[1] + REL[n % 4] + 4, 4)
                row = pl.multiple_of((i * 8 + y * 2 + cores[n // 4]) * 32, 32)
                src = pl.ds(pl.multiple_of(at + slot * 32, 32), 32)
                dst[pl.ds(row, 32), :] = piece[src, :]
            return carry

        lax.fori_loop(0, 2, step, 0)


def halves(part, low_ref, high_ref):
    low_ref[...] = part[0 : TOK // 2, :]
    high_ref[...] = part[TOK // 2 :, :]


def one_kernel(sq_ref, down_ref, low_ref, high_ref):
    halves(down_term(sq_ref, down_ref), low_ref, high_ref)


def two_kernel(sq_ref, down_ref, *refs):
    part_ref = refs[4]

    def step(k, carry):
        part_ref[k] = down_term(sq_ref, down_ref.at[k])
        return carry

    lax.fori_loop(0, 2, step, 0)
    for k in range(2):
        halves(part_ref[k], *refs[2 * k : 2 * k + 2])


def stack_kernel(*refs):
    out, at = refs[-1], 0
    for ref in refs[:-1]:
        out[at : at + ref.shape[0], :] = ref[...]
        at += ref.shape[0]


def smem():
    return pl.BlockSpec(memory_space=pltpu.SMEM)


def vmem():
    return pl.BlockSpec(memory_space=pltpu.VMEM)


def hbm():
    return pl.BlockSpec(memory_space=pl.ANY)


def shape(*dims, dtype=BF):
    return jax.ShapeDtypeStruct(dims, dtype)


def call(body, specs, outs, scratch=(), flops=0, mib=8):
    many = isinstance(outs, (list, tuple))
    return pl.pallas_call(
        body,
        in_specs=specs,
        out_specs=[vmem() for _ in outs] if many else vmem(),
        out_shape=outs,
        scratch_shapes=list(scratch),
        compiler_params=pltpu.CompilerParams(vmem_limit_bytes=mib * 1024 * 1024),
        cost_estimate=pl.CostEstimate(flops=flops, bytes_accessed=0, transcendentals=0),
    )


def local(
    queries,
    keys,
    values,
    output_gate_logits,
    input_gate_log,
    forget_gate_logits,
    extra_decay_log,
    document,
    residual,
    cell_norm_gain,
    output_weight,
    mixer_norm_gain,
    up_weight,
    down_weight,
):
    z, y, c, x = (lax.axis_index(a) for a in ("z", "y", "c", "x"))
    at = jnp.stack([z, y, c, x]).astype(jnp.int32)

    forget_log = jax.nn.log_sigmoid(forget_gate_logits) + extra_decay_log
    docs = document.astype(F32).reshape(NB, BLK)
    gates = jnp.concatenate(
        [input_gate_log.T.reshape(8, BLK), forget_log.T.reshape(8, BLK), docs, docs], axis=0
    )

    own = down_weight.T
    p1, m1 = shift(own, "z", 1), shift(own, "z", -1)
    up_y = [
        up_weight, shift(up_weight, "y", 1), shift(up_weight, "y", -1), shift(up_weight, "y", 2)
    ]

    state, numer, aux = call(
        cell_kernel,
        [vmem()] * 4,
        [shape(288, DH), shape(TOK, 256, dtype=F32), shape(TOK, BLK, dtype=F32)],
        flops=5 * 2 * 10 * 128**3,
    )(gates, queries, keys, values)
    states = [shift_sp(state, by) for by in (1, 2, 3, 4)]

    def to_all(value):
        return [shift(value, "x", by) for by in (1, -1, 2)]

    pack = call(pack_kernel, [smem()] + [vmem()] * 2, shape(256, D))(at, output_weight, residual)
    packs = to_all(pack)
    heads = call(heads_kernel, [vmem()] * 3, shape(384, D))(*packs)
    heads = shift(heads, "c", 1)

    def stack(*pieces):
        rows = sum(piece.shape[0] for piece in pieces)
        return call(stack_kernel, [vmem()] * len(pieces), shape(rows, FF), mib=16)(*pieces)

    pair = shape(64, FF)
    a2, b2 = call(pairs_kernel, [vmem()] * 3, [pair, pair])(own, p1, m1)
    a2, b2 = shift(a2, "z", 2), shift(b2, "z", -2)
    p4 = shift(own, "z", 4)
    ring = call(ring_kernel, [vmem()] * 6, shape(256, FF))(own, p1, m1, p4, a2, b2)
    downs = [ring, shift(ring, "y", 1), shift(ring, "y", -1), shift(ring, "y", 2)]
    other = [ring, stack(*downs[1:3]), downs[3]]
    downs += [shift(a, "c", 1) for a in other]

    up_rows = stack(*up_y)
    u1, d1 = shift(up_rows, "z", 1), shift(up_rows, "z", -1)
    u2, d2 = shift(u1, "z", 1), shift(d1, "z", -1)
    u3, d3 = shift(u2, "z", 1), shift(d2, "z", -1)
    ups = [up_rows, u1, d1, u2, d2, u3, d3, shift(u3, "z", 1)]
    other = [stack(*ups[:5]), stack(*ups[5:7])]
    ups += [shift(a, "c", 1) for a in (*other, ups[7])]

    cells = call(
        combine_kernel,
        [vmem()] * 11,
        shape(TOK + 16, 256),
        [pltpu.VMEM((NB, BLK, BLK), F32)],
        flops=2 * 2 * 512 * 128 * 128,
    )(
        gates,
        queries,
        output_gate_logits,
        cell_norm_gain[None, :],
        mixer_norm_gain.reshape(4, BLK),
        numer,
        aux,
        *states,
    )
    cells = [cells, *to_all(cells)]

    normed, first = call(
        project_kernel,
        [smem()] + [vmem()] * 4 + [hbm()] * 6,
        [shape(TOK, D), shape(TOK, 512)],
        [
            pltpu.VMEM((1024, D), BF),
            pltpu.VMEM((TOK, 1024), BF),
            pltpu.VMEM((4, TOK, 512), BF),
            pltpu.VMEM((4, 8, BLK), F32),
            pltpu.SemaphoreType.DMA,
            pltpu.SemaphoreType.DMA,
        ],
        flops=2 * 512 * 1024 * 2048,
        mib=24,
    )(at, *cells, residual, output_weight, *packs, heads)

    far_down, near_down, own_down = call(
        join_kernel,
        [smem()] + [vmem()] * 7,
        [shape(512, FF), shape(2, 512, FF), shape(512, FF)],
        flops=2**30,
        mib=18,
    )(at, *downs)
    squared = call(
        up_kernel,
        [smem(), vmem()] + [hbm()] * 11,
        shape(TOK, FF),
        [pltpu.VMEM((2, D, 1024), BF), pltpu.SemaphoreType.DMA((2,))],
        flops=2 * 512 * 2048 * 2048,
        mib=14,
    )(at, normed, *ups)

    half_block = shape(TOK // 2, 512)

    def one_call(down):
        return call(
            one_kernel, [vmem()] * 2, [half_block] * 2, flops=2 * 512 * 2048 * 512, mib=12
        )(squared, down)

    far_low, far_high = one_call(far_down)
    far_low, far_high = shift(far_low, "x", 1), shift(far_high, "x", -1)
    right_low, right_high, left_low, left_high = call(
        two_kernel,
        [vmem()] * 2,
        [half_block] * 4,
        [pltpu.VMEM((2, TOK, 512), BF)],
        flops=2 * 512 * 2048 * 1024,
        mib=14,
    )(squared, near_down)
    from_left_high = shift(right_high, "x", 1)
    from_right_low = shift(left_low, "x", -1)
    add = lambda a, b: (a.astype(F32) + b.astype(F32)).astype(BF)
    from_left_low = shift(add(right_low, far_low), "x", 1)
    from_right_high = shift(add(left_high, far_high), "x", -1)
    own_low, own_high = one_call(own_down)
    own_term = jnp.concatenate([own_low, own_high], axis=0)
    from_left = jnp.concatenate([from_left_low, from_left_high], axis=0)
    from_right = jnp.concatenate([from_right_low, from_right_high], axis=0)
    terms = own_term.astype(F32) + from_left.astype(F32) + from_right.astype(F32)
    return (first.astype(F32) + terms).astype(BF)


def solution(mesh):
    split = Mesh(mesh.devices.reshape(8, 4, 2, 4), ("z", "y", "c", "x"))

    return jax.shard_map(
        local,
        mesh=split,
        in_specs=(
            P(SP, "x"),
            P(SP, "x"),
            P(SP, "x"),
            P(SP, "x"),
            P(SP, "x"),
            P(SP, "x"),
            P(SP, "x"),
            P(SP),
            P(SP, "x"),
            P("x"),
            P("x", None),
            P("x"),
            P(SP, "x"),
            P("x", SP),
        ),
        out_specs=P(SP, "x"),
        check_vma=False,
    )
```

```python
import jax
import jax.numpy as jnp
from jax import lax
from jax.experimental import pallas as pl
from jax.experimental.pallas import tpu as pltpu
from jax.sharding import Mesh
from jax.sharding import PartitionSpec as P

NEG = -1e30
EPS = 1e-06
DH = 128
BLK = 128
NB = 4
HD = 2
TOK = 512
D = 2048
FF = 2048
SCALE = DH ** (-0.5)
BF = jnp.bfloat16
F32 = jnp.float32
HIGH = lax.Precision.HIGHEST
SP = ("z", "y", "c")
REL = (0, -1, 1, 2)


def shift(value, axis, by):
    count = lax.axis_size(axis)
    return lax.ppermute(value, axis, [(i, (i + by) % count) for i in range(count)])


def shift_sp(value, by):
    return lax.ppermute(value, SP, [(i, i + by) for i in range(64 - by)])


def split3(value):
    hi = value.astype(BF)
    rest = value - hi.astype(F32)
    mid = rest.astype(BF)
    low = (rest - mid.astype(F32)).astype(BF)
    return hi, mid, low


def block_sums(gates):
    tri = (
        lax.broadcasted_iota(jnp.int32, (BLK, BLK), 0)
        <= lax.broadcasted_iota(jnp.int32, (BLK, BLK), 1)
    ).astype(F32)
    cum = jnp.dot(gates[8:16, :], tri, precision=HIGH, preferred_element_type=F32)
    totals = [cum[r : r + 1, BLK - 1 : BLK] for r in range(8)]
    return cum, totals


def summary_part(gates_ref, k_ref, v_ref, out_ref):
    gates = gates_ref[...]
    cum, totals = block_sums(gates)
    docs = gates[16:24, :]
    last_doc = docs[3:4, BLK - 1 : BLK]
    rows, stabs, sums = [], [], []
    for h in range(HD):
        keeps = []
        after = jnp.zeros((1, 1), F32)
        for b in reversed(range(NB)):
            r = h * NB + b
            keep = (totals[r] - cum[r : r + 1, :]) + after + gates[r : r + 1, :]
            keeps.append(jnp.where(docs[b : b + 1, :] == last_doc, keep, NEG))
            after = after + totals[r]
        keeps = keeps[::-1]
        stab = jnp.max(keeps[0], axis=1, keepdims=True)
        for keep in keeps[1:]:
            stab = jnp.maximum(stab, jnp.max(keep, axis=1, keepdims=True))
        rows += [jnp.exp(keep - stab) for keep in keeps]
        stabs.append(stab)
        sums.append(after)
    columns = jnp.transpose(jnp.concatenate(rows, axis=0))
    norms = []
    for h in range(HD):
        scaled = jnp.concatenate(
            [
                k_ref[b * BLK : (b + 1) * BLK, h * DH : (h + 1) * DH].astype(F32)
                * columns[:, h * NB + b : h * NB + b + 1]
                for b in range(NB)
            ],
            axis=0,
        )
        norms.append(jnp.sum(scaled, axis=0, keepdims=True))
        memory = lax.dot_general(
            scaled.astype(BF),
            v_ref[:, h * DH : (h + 1) * DH],
            (((0,), (0,)), ((), ())),
            preferred_element_type=F32,
        )
        out_ref[h * DH : (h + 1) * DH, :] = memory.astype(BF)
    wide = lambda a: jnp.broadcast_to(a, (1, BLK))
    small = jnp.concatenate(
        norms
        + [wide(a) for a in stabs]
        + [wide(a) for a in sums]
        + [wide(last_doc + 1.0), jnp.zeros((1, BLK), F32)],
        axis=0,
    )
    hi, mid, low = split3(small)
    pad = jnp.zeros((8, BLK), F32)
    out_ref[256:272, :] = jnp.concatenate([hi.astype(F32), mid.astype(F32)], axis=0).astype(BF)
    out_ref[272:288, :] = jnp.concatenate([low.astype(F32), pad], axis=0).astype(BF)


def cell_kernel(gates_ref, q_ref, k_ref, v_ref, state_ref, numer_ref, aux_ref):
    summary_part(gates_ref, k_ref, v_ref, state_ref)
    gates = gates_ref[...]
    cum, totals = block_sums(gates)
    docs = gates[16:24, :]
    cum_cols = jnp.transpose(cum)
    doc_cols = jnp.transpose(docs)
    for b in range(NB):
        width = (b + 1) * BLK
        row_at = lax.broadcasted_iota(jnp.int32, (BLK, width), 0) + b * BLK
        col_at = lax.broadcasted_iota(jnp.int32, (BLK, width), 1)
        doc_row = jnp.concatenate([docs[a : a + 1, :] for a in range(b + 1)], axis=1)
        mask = (doc_cols[:, b : b + 1] == doc_row) & (col_at <= row_at)
        peaks, denoms = [], []
        for h in range(HD):
            r = h * NB + b
            parts = [gates[r : r + 1, :] - cum[r : r + 1, :]]
            between = jnp.zeros((1, 1), F32)
            for a in reversed(range(b)):
                ra = h * NB + a
                parts.append((totals[ra] - cum[ra : ra + 1, :]) + between + gates[ra : ra + 1, :])
                between = between + totals[ra]
            source = jnp.concatenate(parts[::-1], axis=1)
            pair = jnp.where(mask, cum_cols[:, r : r + 1] + source, NEG)
            peak = jnp.max(pair, axis=1, keepdims=True)
            lanes = slice(h * DH, (h + 1) * DH)
            scores = lax.dot_general(
                q_ref[b * BLK : (b + 1) * BLK, lanes],
                k_ref[0:width, lanes],
                (((1,), (1,)), ((), ())),
                preferred_element_type=F32,
            )
            scores = scores * SCALE * jnp.exp(pair - peak)
            denoms.append(jnp.sum(scores, axis=1, keepdims=True))
            peaks.append(peak)
            numer_ref[b * BLK : (b + 1) * BLK, lanes] = jnp.dot(
                scores.astype(BF), v_ref[0:width, lanes], preferred_element_type=F32
            )
        lane = lax.broadcasted_iota(jnp.int32, (BLK, BLK), 1)
        aux = jnp.where(
            lane == 0,
            peaks[0],
            jnp.where(lane == 1, peaks[1], jnp.where(lane == 2, denoms[0], denoms[1])),
        )
        aux_ref[b * BLK : (b + 1) * BLK, :] = aux


def combine_kernel(
    gates_ref, q_ref, og_ref, gain_ref, mixer_gain, numer_ref, aux_ref, s1, s2, s3, s4, full_ref, far_ref
):
    gates = gates_ref[...]
    cum, totals = block_sums(gates)
    docs = gates[16:24, :]
    cum_cols = jnp.transpose(cum)
    doc_cols = jnp.transpose(docs)
    doc0 = docs[0:1, 0:1]
    smalls = []
    for s in (s1, s2, s3, s4):
        upper = s[256:272, :].astype(F32)
        lower = s[272:288, :].astype(F32)
        smalls.append(upper[0:8, :] + upper[8:16, :] + lower[0:8, :])
    states = []
    for h in range(HD):
        far = jnp.zeros((1, 1), F32)
        logs, valids = [], []
        for small in smalls:
            valid = small[6:7, 0:1] == doc0 + 1.0
            logs.append(jnp.where(valid, small[2 + h : 3 + h, 0:1] + far, NEG))
            valids.append(valid)
            far = far + small[4 + h : 5 + h, 0:1]
        stab = jnp.maximum(jnp.maximum(logs[0], logs[1]), jnp.maximum(logs[2], logs[3]))
        memory = jnp.zeros((DH, DH), F32)
        normer = jnp.zeros((1, DH), F32)
        for s, small, log, valid in zip((s1, s2, s3, s4), smalls, logs, valids):
            weight = jnp.where(valid, jnp.exp(log - stab), 0.0)
            memory = memory + weight * s[h * DH : (h + 1) * DH, :].astype(F32)
            normer = normer + weight * small[h : h + 1, :]
        states.append((memory.astype(BF), normer, stab))
    before = [jnp.zeros((1, 1), F32) for _ in range(HD)]
    lane = lax.broadcasted_iota(jnp.int32, (BLK, BLK), 1)
    for b in range(NB):
        live = doc_cols[:, b : b + 1] == doc0
        far = []
        for h in range(HD):
            r = h * NB + b
            stab = states[h][2]
            log = cum_cols[:, r : r + 1] + (before[h] + stab)
            far.append(jnp.where(live & (stab > 0.5 * NEG), log, NEG))
            before[h] = before[h] + totals[r]
        far_ref[b] = jnp.where(lane == 0, far[0], far[1])

    def step(b, table):
        rows = pl.ds(pl.multiple_of(b * BLK, BLK), BLK)
        aux = aux_ref[rows, :]
        logs = far_ref[b]
        squares = jnp.zeros((BLK, 1), F32)
        for h in range(HD):
            lanes = slice(h * DH, (h + 1) * DH)
            memory, normer, _ = states[h]
            carried = logs[:, h : h + 1]
            peak = aux[:, h : h + 1]
            merged = jnp.maximum(peak, carried)
            own_w = jnp.exp(peak - merged)
            far_w = jnp.exp(carried - merged) * SCALE
            q_blk = q_ref[rows, lanes]
            numer = own_w * numer_ref[rows, lanes] + far_w * jnp.dot(
                q_blk, memory, preferred_element_type=F32
            )
            denom = own_w * aux[:, 2 + h : 3 + h] + far_w * jnp.sum(
                q_blk.astype(F32) * normer, axis=1, keepdims=True
            )
            cell = numer / jnp.maximum(jnp.abs(denom), 1.0)
            squares = squares + jnp.sum(cell * cell, axis=1, keepdims=True)
            gate = jax.nn.sigmoid(og_ref[rows, lanes].astype(F32))
            full_ref[rows, lanes] = (gate * cell * gain_ref[0:1, lanes].astype(F32)).astype(BF)
        return jnp.where(lane == b, squares, table)

    table = lax.fori_loop(0, NB, step, jnp.zeros((BLK, BLK), F32))
    hi, mid, low = (a.astype(F32) for a in split3(jnp.transpose(table)[0:8, :]))
    full_ref[TOK : TOK + 16, 0:128] = jnp.concatenate([hi, low], axis=0).astype(BF)
    gain = jnp.concatenate([mixer_gain[...].astype(F32), jnp.zeros((4, BLK), F32)], axis=0)
    full_ref[TOK : TOK + 16, 128:256] = jnp.concatenate([mid, gain], axis=0).astype(BF)


def block_of(at_ref, rel):
    return lax.rem(at_ref[3] + rel + 4, 4)


def project_kernel(at_ref, *refs):
    cells, own_resid, own_w = refs[0:4], refs[4], refs[5]
    packs, other = refs[6:9], refs[9]
    normed_ref, own_ref, w_ref, g_ref, r_ref, gain_ref, w_sem, r_sem = refs[10:]
    core = at_ref[2]
    weights = [pltpu.make_async_copy(own_w, w_ref.at[pl.ds(0, 256)], w_sem)]
    rows = [pltpu.make_async_copy(own_resid, r_ref.at[block_of(at_ref, 0)], r_sem)]
    for k, pack in enumerate(packs):
        parts = ((pack, 0, core), (other, k * 128, 1 - core))
        for part, at, half in parts:
            start = pl.multiple_of((k + 1) * 256 + half * 128, 128)
            weights.append(
                pltpu.make_async_copy(
                    part.at[pl.ds(at, 128)], w_ref.at[pl.ds(start, 128)], w_sem
                )
            )
        for i in range(4):
            rows.append(
                pltpu.make_async_copy(
                    pack.at[pl.ds(128, 128), pl.ds(i * 512, 512)],
                    r_ref.at[block_of(at_ref, REL[k + 1]), pl.ds(i * 128, 128)],
                    r_sem,
                )
            )
    for copy in weights + rows:
        copy.start()
    squares = jnp.zeros((8, BLK), F32)
    for k, rel in enumerate(REL):
        g_ref[:, k * 256 : (k + 1) * 256] = cells[k][0:TOK, :]
        left = cells[k][TOK : TOK + 16, 0:128].astype(F32)
        right = cells[k][TOK : TOK + 16, 128:256].astype(F32)
        squares = squares + (left[0:8, :] + right[0:8, :] + left[8:16, :])
        gain_ref[block_of(at_ref, rel)] = right[8:16, :]
    columns = jnp.transpose(lax.rsqrt(squares / 1024.0 + EPS))
    inverse = jnp.concatenate([columns[:, b : b + 1] for b in range(NB)], axis=0)
    for copy in weights + rows:
        copy.wait()

    def step(a, total):
        cols = pl.ds(pl.multiple_of(a * 512, 512), 512)
        head = jnp.dot(g_ref[...], w_ref[:, cols], preferred_element_type=F32) * inverse
        first = (r_ref[a].astype(F32) + head).astype(BF)
        r_ref[a] = first
        wide = first.astype(F32)
        return total + jnp.sum(wide * wide, axis=1, keepdims=True)

    total = lax.fori_loop(0, 4, step, jnp.zeros((TOK, 1), F32))
    own_ref[...] = r_ref[block_of(at_ref, 0)]
    inverse = lax.rsqrt(total / float(D) + EPS)

    def scale(a, carry):
        gain = gain_ref[a]
        gain = jnp.concatenate([gain[i : i + 1, :] for i in range(4)], axis=1)
        cols = pl.ds(pl.multiple_of(a * 512, 512), 512)
        normed_ref[:, cols] = (r_ref[a].astype(F32) * inverse * gain).astype(BF)
        return carry

    lax.fori_loop(0, 4, scale, 0)


def pack_kernel(at_ref, weight_ref, resid_ref, out_ref):
    start = pl.multiple_of(at_ref[2] * 128, 128)
    out_ref[0:128, :] = weight_ref[pl.ds(start, 128), :]
    for i in range(4):
        out_ref[128:256, i * 512 : (i + 1) * 512] = resid_ref[i * 128 : (i + 1) * 128, :]


def heads_kernel(a, b, c, out_ref):
    for k, ref in enumerate((a, b, c)):
        out_ref[k * 128 : (k + 1) * 128, :] = ref[0:128, :]


def pairs_kernel(own, p1, m1, a_ref, b_ref):
    a_ref[0:32, :] = own[...]
    a_ref[32:64, :] = p1[...]
    b_ref[0:32, :] = own[...]
    b_ref[32:64, :] = m1[...]


def ring_kernel(own, p1, m1, p4, a, b, out):
    for k, piece in enumerate((own, p1, m1, p4)):
        out[k * 32 : (k + 1) * 32, :] = piece[...]
    out[128:192, :] = a[...]
    out[192:256, :] = b[...]


def shard_row(at_ref, dz, dy, core):
    z, y = lax.rem(at_ref[0] + dz + 8, 8), lax.rem(at_ref[1] + dy + 4, 4)
    return pl.multiple_of((z * 8 + y * 2 + core) * 32, 32)


def wait_all(dst, sem):
    pltpu.make_async_copy(dst, dst, sem).wait()


def up_kernel(at_ref, x_ref, *refs):
    own, other = refs[:8], refs[8:11]
    sq_ref, up_ref, sems = refs[11:]
    cores = (at_ref[2], 1 - at_ref[2])

    pieces = [(piece, 0) for piece in own]
    pieces += [(other[n], 128 * k) for n, count in enumerate((5, 2, 1)) for k in range(count)]

    def start(n, carry):
        f, k = n // 4, lax.rem(n, 4)
        cols = pl.ds(pl.multiple_of(f * 1024, 1024), 1024)
        dy = jnp.where(k == 0, 0, jnp.where(k == 1, -1, k - 1))
        for i, (piece, at) in enumerate(pieces):
            row = shard_row(at_ref, (0, -1, 1, -2, 2, -3, 3, 4)[i % 8], dy, cores[i // 8])
            pltpu.make_async_copy(
                piece.at[pl.ds(pl.multiple_of(at + k * 32, 32), 32), cols],
                up_ref.at[f, pl.ds(row, 32)],
                sems.at[f],
            ).start()
        return carry

    lax.fori_loop(0, 8, start, 0)

    def step(f, carry):
        @pl.when(lax.rem(f, 2) == 0)
        def _():
            wait_all(up_ref.at[f // 2], sems.at[f // 2])

        part = up_ref[f // 2, :, pl.ds(pl.multiple_of(lax.rem(f, 2) * 512, 512), 512)]
        hidden = jnp.dot(x_ref[...], part, preferred_element_type=F32)
        cols = pl.ds(pl.multiple_of(f * 512, 512), 512)
        sq_ref[:, cols] = jnp.square(jnp.maximum(hidden, 0.0)).astype(BF)
        return carry

    lax.fori_loop(0, 4, step, 0)


def down_term(sq_ref, down_ref):
    part = jnp.zeros((TOK, 512), F32)
    for f in range(4):
        cols = slice(f * 512, (f + 1) * 512)
        part = part + lax.dot_general(
            sq_ref[:, cols],
            down_ref[:, cols],
            (((1,), (1,)), ((), ())),
            preferred_element_type=F32,
        )
    return part.astype(BF)


def join_kernel(at_ref, *refs):
    far_ref, near_ref, last_ref = refs[6:]
    own, (other, other_far) = refs[:4], refs[4:6]
    pieces = [(piece, 0) for piece in own]
    pieces += [(other, 0), (other, 256), (other, 512), (other_far, 0)]
    cores = (at_ref[2], 1 - at_ref[2])
    outs = (far_ref, near_ref.at[0], near_ref.at[1], last_ref)
    for rel, dst in zip((2, 1, -1, 0), outs):
        block = block_of(at_ref, rel)

        def step(i, carry, dst=dst, block=block):
            dz = lax.rem(block * 2 + i - at_ref[0] + 8, 8)
            slot = jnp.int32(0)
            for at, key in enumerate((0, 7, 1, 4, 6, 5, 2, 3)):
                slot = jnp.where(dz == key, at, slot)
            for n, (piece, at) in enumerate(pieces):
                y = lax.rem(at_ref[1] + REL[n % 4] + 4, 4)
                row = pl.multiple_of((i * 8 + y * 2 + cores[n // 4]) * 32, 32)
                src = pl.ds(pl.multiple_of(at + slot * 32, 32), 32)
                dst[pl.ds(row, 32), :] = piece[src, :]
            return carry

        lax.fori_loop(0, 2, step, 0)


def halves(part, low_ref, high_ref):
    low_ref[...] = part[0 : TOK // 2, :]
    high_ref[...] = part[TOK // 2 :, :]


def one_kernel(sq_ref, down_ref, low_ref, high_ref):
    halves(down_term(sq_ref, down_ref), low_ref, high_ref)


def two_kernel(sq_ref, down_ref, *refs):
    part_ref = refs[4]

    def step(k, carry):
        part_ref[k] = down_term(sq_ref, down_ref.at[k])
        return carry

    lax.fori_loop(0, 2, step, 0)
    for k in range(2):
        halves(part_ref[k], *refs[2 * k : 2 * k + 2])


def stack_kernel(*refs):
    out, at = refs[-1], 0
    for ref in refs[:-1]:
        out[at : at + ref.shape[0], :] = ref[...]
        at += ref.shape[0]


def smem():
    return pl.BlockSpec(memory_space=pltpu.SMEM)


def vmem():
    return pl.BlockSpec(memory_space=pltpu.VMEM)


def hbm():
    return pl.BlockSpec(memory_space=pl.ANY)


def shape(*dims, dtype=BF):
    return jax.ShapeDtypeStruct(dims, dtype)


def call(body, specs, outs, scratch=(), flops=0, mib=8):
    many = isinstance(outs, (list, tuple))
    return pl.pallas_call(
        body,
        in_specs=specs,
        out_specs=[vmem() for _ in outs] if many else vmem(),
        out_shape=outs,
        scratch_shapes=list(scratch),
        compiler_params=pltpu.CompilerParams(vmem_limit_bytes=mib * 1024 * 1024),
        cost_estimate=pl.CostEstimate(flops=flops, bytes_accessed=0, transcendentals=0),
    )


def local(
    queries,
    keys,
    values,
    output_gate_logits,
    input_gate_log,
    forget_gate_logits,
    extra_decay_log,
    document,
    residual,
    cell_norm_gain,
    output_weight,
    mixer_norm_gain,
    up_weight,
    down_weight,
):
    z, y, c, x = (lax.axis_index(a) for a in ("z", "y", "c", "x"))
    at = jnp.stack([z, y, c, x]).astype(jnp.int32)

    forget_log = jax.nn.log_sigmoid(forget_gate_logits) + extra_decay_log
    docs = document.astype(F32).reshape(NB, BLK)
    gates = jnp.concatenate(
        [input_gate_log.T.reshape(8, BLK), forget_log.T.reshape(8, BLK), docs, docs], axis=0
    )

    own = down_weight.T
    p1, m1 = shift(own, "z", 1), shift(own, "z", -1)
    up_y = [
        up_weight, shift(up_weight, "y", 1), shift(up_weight, "y", -1), shift(up_weight, "y", 2)
    ]

    state, numer, aux = call(
        cell_kernel,
        [vmem()] * 4,
        [shape(288, DH), shape(TOK, 256, dtype=F32), shape(TOK, BLK, dtype=F32)],
        flops=5 * 2 * 10 * 128**3,
    )(gates, queries, keys, values)
    states = [shift_sp(state, by) for by in (1, 2, 3, 4)]

    def to_all(value):
        return [shift(value, "x", by) for by in (1, -1, 2)]

    pack = call(pack_kernel, [smem()] + [vmem()] * 2, shape(256, D))(at, output_weight, residual)
    packs = to_all(pack)
    heads = call(heads_kernel, [vmem()] * 3, shape(384, D))(*packs)
    heads = shift(heads, "c", 1)

    def stack(*pieces):
        rows = sum(piece.shape[0] for piece in pieces)
        return call(stack_kernel, [vmem()] * len(pieces), shape(rows, FF), mib=16)(*pieces)

    pair = shape(64, FF)
    a2, b2 = call(pairs_kernel, [vmem()] * 3, [pair, pair])(own, p1, m1)
    a2, b2 = shift(a2, "z", 2), shift(b2, "z", -2)
    p4 = shift(own, "z", 4)
    ring = call(ring_kernel, [vmem()] * 6, shape(256, FF))(own, p1, m1, p4, a2, b2)
    downs = [ring, shift(ring, "y", 1), shift(ring, "y", -1)]
    far = shift(downs[1][:128], "y", 1), shift(downs[2][128:], "y", -1)
    downs += [stack(*far)]
    other = [stack(*downs[:3]), downs[3]]
    downs += [shift(a, "c", 1) for a in other]

    up_rows = stack(*up_y)
    u1, d1 = shift(up_rows, "z", 1), shift(up_rows, "z", -1)
    u2, d2 = shift(u1, "z", 1), shift(d1, "z", -1)
    u3, d3 = shift(u2, "z", 1), shift(d2, "z", -1)
    ups = [up_rows, u1, d1, u2, d2, u3, d3, shift(u3, "z", 1)]
    other = [stack(*ups[:5]), stack(*ups[5:7])]
    ups += [shift(a, "c", 1) for a in (*other, ups[7])]

    cells = call(
        combine_kernel,
        [vmem()] * 11,
        shape(TOK + 16, 256),
        [pltpu.VMEM((NB, BLK, BLK), F32)],
        flops=2 * 2 * 512 * 128 * 128,
    )(
        gates,
        queries,
        output_gate_logits,
        cell_norm_gain[None, :],
        mixer_norm_gain.reshape(4, BLK),
        numer,
        aux,
        *states,
    )
    cells = [cells, *to_all(cells)]

    normed, first = call(
        project_kernel,
        [smem()] + [vmem()] * 4 + [hbm()] * 6,
        [shape(TOK, D), shape(TOK, 512)],
        [
            pltpu.VMEM((1024, D), BF),
            pltpu.VMEM((TOK, 1024), BF),
            pltpu.VMEM((4, TOK, 512), BF),
            pltpu.VMEM((4, 8, BLK), F32),
            pltpu.SemaphoreType.DMA,
            pltpu.SemaphoreType.DMA,
        ],
        flops=2 * 512 * 1024 * 2048,
        mib=24,
    )(at, *cells, residual, output_weight, *packs, heads)

    far_down, near_down, own_down = call(
        join_kernel,
        [smem()] + [vmem()] * 6,
        [shape(512, FF), shape(2, 512, FF), shape(512, FF)],
        flops=2**30,
        mib=18,
    )(at, *downs)
    squared = call(
        up_kernel,
        [smem(), vmem()] + [hbm()] * 11,
        shape(TOK, FF),
        [pltpu.VMEM((2, D, 1024), BF), pltpu.SemaphoreType.DMA((2,))],
        flops=2 * 512 * 2048 * 2048,
        mib=14,
    )(at, normed, *ups)

    half_block = shape(TOK // 2, 512)

    def one_call(down):
        return call(
            one_kernel, [vmem()] * 2, [half_block] * 2, flops=2 * 512 * 2048 * 512, mib=12
        )(squared, down)

    far_low, far_high = one_call(far_down)
    far_low, far_high = shift(far_low, "x", 1), shift(far_high, "x", -1)
    right_low, right_high, left_low, left_high = call(
        two_kernel,
        [vmem()] * 2,
        [half_block] * 4,
        [pltpu.VMEM((2, TOK, 512), BF)],
        flops=2 * 512 * 2048 * 1024,
        mib=14,
    )(squared, near_down)
    from_left_high = shift(right_high, "x", 1)
    from_right_low = shift(left_low, "x", -1)
    add = lambda a, b: (a.astype(F32) + b.astype(F32)).astype(BF)
    from_left_low = shift(add(right_low, far_low), "x", 1)
    from_right_high = shift(add(left_high, far_high), "x", -1)
    own_low, own_high = one_call(own_down)
    own_term = jnp.concatenate([own_low, own_high], axis=0)
    from_left = jnp.concatenate([from_left_low, from_left_high], axis=0)
    from_right = jnp.concatenate([from_right_low, from_right_high], axis=0)
    terms = own_term.astype(F32) + from_left.astype(F32) + from_right.astype(F32)
    return (first.astype(F32) + terms).astype(BF)


def solution(mesh):
    split = Mesh(mesh.devices.reshape(8, 4, 2, 4), ("z", "y", "c", "x"))

    return jax.shard_map(
        local,
        mesh=split,
        in_specs=(
            P(SP, "x"),
            P(SP, "x"),
            P(SP, "x"),
            P(SP, "x"),
            P(SP, "x"),
            P(SP, "x"),
            P(SP, "x"),
            P(SP),
            P(SP, "x"),
            P("x"),
            P("x", None),
            P("x"),
            P(SP, "x"),
            P("x", SP),
        ),
        out_specs=P(SP, "x"),
        check_vma=False,
    )
```
